512 devices in a mesh: fs: 16 (over z), rep: 4 (over y), tp: 8 (over x, core).
Axes of the slice: x: 4, y: 4, z: 16, core: 2. Of those that a mesh axis runs over, the one named last changes fastest.
Arguments:
- normed: bfloat16 [40960, 2048], P(('fs', 'rep')), may hold values from -150 to 150
- rec_cot: bfloat16 [40960, 2048], P(('fs', 'rep'), 'tp'), may hold values from -0.74115883 to 0.74115883
- conv_out: bfloat16 [40960, 2048], P(('fs', 'rep'), 'tp'), may hold values from -6 to 6
- gate_cot: bfloat16 [40960, 2048], P(('fs', 'rep'), 'tp'), may hold values from -0.029541016 to 0.029541016
- rec_weight: float32 [2048, 2048], P('fs', 'tp'), may hold values from -0.125 to 0.125
- rec_moment: float32 [2048, 2048], P('fs', 'tp'), may hold values from -6 to 6
- rec_right: bfloat16 [2048, 256], P('tp'), may hold values from -1 to 2
- gate_weight: float32 [8, 256, 256], P('tp', 'fs'), may hold values from -0.375 to 0.375
- gate_moment: float32 [8, 256, 256], P('tp', 'fs'), may hold values from -6 to 6
- gate_left: bfloat16 [8, 256, 256], P('tp', 'fs'), may hold values from -1 to 2
- gate_right: bfloat16 [8, 256, 256], P('tp'), may hold values from -1 to 2
Outputs:
- rec_weight_new: float32 [2048, 2048], P('fs', 'tp')
- rec_moment_new: float32 [2048, 2048], P('fs', 'tp')
- rec_step: float32 [2048, 2048], P('fs', 'tp')
- rec_copy: bfloat16 [2048, 2048], P('fs', 'tp')
- gate_weight_new: float32 [8, 256, 256], P('tp', 'fs')
- gate_moment_new: float32 [8, 256, 256], P('tp', 'fs')
- gate_step: float32 [8, 256, 256], P('tp', 'fs')
- gate_copy: bfloat16 [8, 256, 256], P('tp', 'fs')
The draws below stay inside these ranges and needn't reach their ends.
All inputs are finite; a program needn't handle non-finite values.
Results may differ from the reference program's by a relative error of at most 0.001.
Values sent between devices are 32-bit elements; how exact they have to be, the bound alone decides.
No kernel may reach another device: no remote copies, remote signals or barrier semaphores. Data moves between devices by JAX's collectives and lax.ppermute only.
A program may use at most 64 MiB of HBM per device.

```python
import jax
import jax.numpy as jnp
from jax import lax

D = 2048
D_RNN = 2048
HEADS = 8
BLK = 256
TOKENS = 40960


def rising_scales(key, column_count):
    position = jnp.arange(column_count, dtype=jnp.float32) / column_count
    jitter = jnp.exp(jax.random.uniform(key, (column_count,), jnp.float32, 0.0, jnp.log(3.0)))
    return jnp.exp(jnp.log(4.0) * position) * jitter


def token_matrix(key, column_count, overall):
    key_list = jax.random.split(key, 2)
    scales = rising_scales(key_list[0], column_count) * overall
    values = jnp.clip(jax.random.normal(key_list[1], (TOKENS, column_count), jnp.float32), -6.0, 6.0)
    return values * scales


def identity_plus(key, count, block_size):
    noise = jnp.clip(jax.random.normal(key, (count, block_size, block_size), jnp.float32), -4.0, 4.0)
    symmetric = (noise + jnp.swapaxes(noise, 1, 2)) * (0.5 / jnp.sqrt(2.0 * block_size))
    result = jnp.eye(block_size, dtype=jnp.float32)[None] + symmetric
    return jnp.clip(result, -1.0, 2.0)


def draw_normed(key, part):
    return token_matrix(jax.random.fold_in(key, 11), D, 1.0).astype(jnp.bfloat16)


def draw_rec_cot(key, part):
    return token_matrix(jax.random.fold_in(key, 12), D_RNN, TOKENS ** (-0.5)).astype(jnp.bfloat16)


def draw_rec_right(key, part):
    blocks = identity_plus(jax.random.fold_in(key, 13), D_RNN // BLK, BLK)
    return blocks.reshape(D_RNN, BLK).astype(jnp.bfloat16)


def draw_gate_left(key, part):
    return identity_plus(jax.random.fold_in(key, 14), HEADS, BLK).astype(jnp.bfloat16)


def draw_gate_right(key, part):
    return identity_plus(jax.random.fold_in(key, 15), HEADS, BLK).astype(jnp.bfloat16)


def steps_of(stream_key, dims, pieces, low, high):
    loudness, own = 1.0, jax.random.fold_in(stream_key, 6)
    for dim, parts in pieces:
        draws = jnp.exp(jax.random.uniform(jax.random.fold_in(own, dim), (parts,), jnp.float32, low / len(pieces), high / len(pieces)))
        loudness = loudness * jnp.repeat(draws, dims[dim] // parts).reshape([-1 if axis == dim else 1 for axis in range(len(dims))])
    return loudness


def scatter_about(own_key, extent, scale, bound, pieces=(), kind=jnp.bfloat16):
    values = scale * jax.random.normal(own_key, extent, jnp.float32)
    if pieces:
        values = values * steps_of(own_key, extent, pieces, -0.22, 0.18)
    return jnp.clip(values, -bound, bound).astype(kind)


def setup_inputs(seed: int = 0) -> dict:
    splits = jax.random.split(jax.random.key(seed), 12)
    return {
        "normed": draw_normed(jax.random.fold_in(splits[11], 71), 0),
        "rec_cot": draw_rec_cot(jax.random.fold_in(splits[11], 71), 0),
        "conv_out": scatter_about(splits[2], (TOKENS, D_RNN), 1.0, 6.0, ((0, 64), (1, 8))),
        "gate_cot": scatter_about(splits[3], (TOKENS, D_RNN), (TOKENS ** -0.5), 0.029541016, ((0, 64), (1, 8))),
        "rec_weight": scatter_about(splits[4], (D, D_RNN), D ** -0.5, 0.125, ((0, 16), (1, 8)), jnp.float32),
        "rec_moment": scatter_about(splits[5], (D, D_RNN), 1.0, 6.0, ((0, 16), (1, 8)), jnp.float32),
        "rec_right": draw_rec_right(jax.random.fold_in(splits[11], 71), 0),
        "gate_weight": scatter_about(splits[7], (HEADS, BLK, BLK), BLK ** -0.5, 0.375, ((0, 8), (1, 16)), jnp.float32),
        "gate_moment": scatter_about(splits[8], (HEADS, BLK, BLK), 1.0, 6.0, ((0, 8), (1, 16)), jnp.float32),
        "gate_left": draw_gate_left(jax.random.fold_in(splits[11], 71), 0),
        "gate_right": draw_gate_right(jax.random.fold_in(splits[11], 71), 0),
    }


BETA = 0.9
LEARN_RATE = 0.02
EPSILON = 1e-06

def precondition_right(gradient, factor):
    row_count = gradient.shape[0]
    block_size = factor.shape[1]
    blocks = factor.shape[0] // block_size
    shaped = gradient.reshape(row_count, blocks, block_size)
    factors = factor.astype(jnp.float32).reshape(blocks, block_size, block_size)
    result = jnp.einsum('rbi,bij->rbj', shaped, factors, precision=lax.Precision.HIGHEST)
    return result.reshape(row_count, blocks * block_size)

def apply_update(weight, moment, precond, gradient):
    new_moment = BETA * moment + precond
    scale = jnp.sqrt(jnp.sum(gradient * gradient)) / jnp.sqrt(jnp.sum(new_moment * new_moment) + EPSILON)
    step_taken = LEARN_RATE * scale * new_moment
    new_weight = weight - step_taken
    return (new_weight, new_moment, step_taken, new_weight.astype(jnp.bfloat16))

def reference(normed, rec_cot, conv_out, gate_cot, rec_weight, rec_moment, rec_right, gate_weight, gate_moment, gate_left, gate_right):
    rec_grad = lax.dot_general(normed, rec_cot, (((0,), (0,)), ((), ())), preferred_element_type=jnp.float32)
    rec_pre = precondition_right(rec_grad, rec_right)
    conv_blocks = conv_out.astype(jnp.float32).reshape(TOKENS, HEADS, BLK)
    cot_blocks = gate_cot.astype(jnp.float32).reshape(TOKENS, HEADS, BLK)
    gate_grad = jnp.einsum('thi,thj->hij', conv_blocks, cot_blocks)
    right_done = jnp.einsum('hij,hjk->hik', gate_grad, gate_right.astype(jnp.float32), precision=lax.Precision.HIGHEST)
    gate_pre = jnp.einsum('hij,hjk->hik', gate_left.astype(jnp.float32), right_done, precision=lax.Precision.HIGHEST)
    rec_new, rec_mom, rec_taken, rec_low = apply_update(rec_weight, rec_moment, rec_pre, rec_grad)
    gate_new, gate_mom, gate_taken, gate_low = apply_update(gate_weight, gate_moment, gate_pre, gate_grad)
    return (rec_new, rec_mom, rec_taken, rec_low, gate_new, gate_mom, gate_taken, gate_low)
```

```python
import jax
import jax.numpy as jnp
from jax import lax
from jax.sharding import Mesh
from jax.sharding import PartitionSpec as P

FS = ("fs_hi", "fs_lo")
NEAR = ("fs_lo", "rep")
TP = ("tp_0", "tp_1")

BETA = 0.9
LEARN_RATE = 0.02
EPSILON = 1e-06
F32 = jnp.float32
HIGH = lax.Precision.HIGHEST


def size_of(axes):
    axes = (axes,) if isinstance(axes, str) else axes
    size = 1
    for axis in axes:
        size *= lax.axis_size(axis)
    return size


def exchange(tiles, axes):
    return lax.all_to_all(tiles, axes, split_axis=0, concat_axis=0, tiled=True)


def gathered(value, axes):
    copies = jnp.broadcast_to(value, (size_of(axes), *value.shape))
    return exchange(copies, axes)


def by_owner(rows, hi, lo, rep):
    columns = rows.shape[-1]
    tiles = rows.reshape(hi, lo, rep, -1, columns)
    return tiles.transpose(1, 2, 0, 3, 4).reshape(lo * rep, hi, -1, columns)


def shards(
    normed,
    rec_cot,
    conv_out,
    gate_cot,
    rec_weight,
    rec_moment,
    rec_right,
    gate_weight,
    gate_moment,
    gate_left,
    gate_right,
):
    hi, lo = lax.axis_size("fs_hi"), lax.axis_size("fs_lo")
    rep = lax.axis_size("rep")
    fs = hi * lo
    block = gate_weight.shape[-1]

    left_rows = gate_left[0].astype(F32)
    left = gathered(left_rows, FS).reshape(block, block)

    contract = (((0,), (0,)), ((), ()))
    rec_part = lax.dot_general(normed, rec_cot, contract, preferred_element_type=F32)
    gate_part = lax.dot_general(conv_out, gate_cot, contract, preferred_element_type=F32)
    right = gate_right[0].astype(F32)
    pre_part = jnp.dot(
        jnp.dot(left, gate_part, precision=HIGH), right, precision=HIGH
    )

    tiles = jnp.concatenate(
        [by_owner(v, hi, lo, rep) for v in (rec_part, gate_part, pre_part)], axis=2
    )
    near = exchange(tiles, NEAR).sum(axis=0)
    own = exchange(near, "fs_hi").sum(axis=0)

    full = gathered(own, "rep")
    n_rec, n_gate = rec_part.shape[0] // (fs * rep), block // (fs * rep)
    rec_grad = full[:, :n_rec].reshape(-1, block)
    gate_grad = full[:, n_rec : n_rec + n_gate].reshape(-1, block)
    gate_pre = full[:, n_rec + n_gate :].reshape(-1, block)

    rec_pre = jnp.dot(rec_grad, rec_right.astype(F32), precision=HIGH)
    rec_moment_new = BETA * rec_moment + rec_pre
    gate_moment_new = BETA * gate_moment[0] + gate_pre
    sums = jnp.stack(
        [
            jnp.sum(v * v)
            for v in (rec_grad, rec_moment_new, gate_grad, gate_moment_new)
        ]
    )
    sums = jnp.broadcast_to(sums[:, None], (4, 128))
    sums = gathered(sums, FS).sum(axis=0)
    totals = gathered(sums, TP).sum(axis=0)[:, 0]
    rec_scale = jnp.sqrt(totals[0]) / jnp.sqrt(totals[1] + EPSILON)
    gate_scale = jnp.sqrt(totals[2]) / jnp.sqrt(totals[3] + EPSILON)
    rec_taken = LEARN_RATE * rec_scale * rec_moment_new
    gate_taken = LEARN_RATE * gate_scale * gate_moment_new
    rec_new = rec_weight - rec_taken
    gate_new = gate_weight[0] - gate_taken
    return (
        rec_new,
        rec_moment_new,
        rec_taken,
        rec_new.astype(jnp.bfloat16),
        gate_new[None],
        gate_moment_new[None],
        gate_taken[None],
        gate_new.astype(jnp.bfloat16)[None],
    )


def solution(mesh):
    fs, rep, tp = (mesh.shape[name] for name in ("fs", "rep", "tp"))
    split = Mesh(
        mesh.devices.reshape(fs // 2, 2, rep, tp // 2, 2),
        (*FS, "rep", *TP),
    )
    tokens = (*FS, "rep")
    placed = (
        P(tokens, None),
        P(tokens, TP),
        P(tokens, TP),
        P(tokens, TP),
        P(FS, TP),
        P(FS, TP),
        P(TP, None),
        P(TP, FS, None),
        P(TP, FS, None),
        P(TP, FS, None),
        P(TP, None, None),
    )
    return jax.shard_map(
        shards,
        mesh=split,
        in_specs=placed,
        out_specs=(P(FS, TP),) * 4 + (P(TP, FS, None),) * 4,
        check_vma=False,
    )
```

```python
import jax
import jax.numpy as jnp
from jax import lax
from jax.experimental import pallas as pl
from jax.experimental.pallas import tpu as pltpu
from jax.sharding import Mesh
from jax.sharding import PartitionSpec as P

TP = ("tp_0", "tp_1")

BETA = 0.9
LEARN_RATE = 0.02
EPSILON = 1e-06
GROUPS = 4
GRANT = 16 << 20
F32 = jnp.float32
HIGH = lax.Precision.HIGHEST
ALONG_ROWS = (((0,), (0,)), ((), ()))
ALONG_COLUMNS = (((1,), (1,)), ((), ()))


def size_of(axes):
    axes = (axes,) if isinstance(axes, str) else axes
    size = 1
    for axis in axes:
        size *= lax.axis_size(axis)
    return size


def exchange(tiles, axes):
    return lax.all_to_all(tiles, axes, split_axis=0, concat_axis=0, tiled=True)


def whole():
    return pl.BlockSpec(memory_space=pltpu.VMEM)


def on_core(kernel, outs, args, scratch=(), flops=1 << 26):
    moved = sum(a.size * a.dtype.itemsize for a in (*args, *outs))
    single = len(outs) == 1
    return pl.pallas_call(
        kernel,
        out_shape=outs[0] if single else outs,
        in_specs=[whole() for _ in args],
        out_specs=whole() if single else [whole() for _ in outs],
        scratch_shapes=list(scratch),
        compiler_params=pltpu.CompilerParams(vmem_limit_bytes=GRANT),
        cost_estimate=pl.CostEstimate(
            flops=flops, bytes_accessed=moved, transcendentals=0
        ),
    )(*args)


def product_kernel(normed, rec_cot, conv_out, gate_cot, tiles, turned):
    rep, rows, _ = tiles.shape
    group = pl.program_id(0)

    @pl.when(group == 0)
    def _():
        turned[...] = lax.dot_general(
            gate_cot[...], conv_out[...], ALONG_ROWS, preferred_element_type=F32
        )

    part = lax.dot_general(
        normed[...], rec_cot[...], ALONG_ROWS, preferred_element_type=F32
    )
    share = turned.shape[0] // rep
    piece = share // GROUPS
    rec_rows = rows - piece
    owners = rec_rows * rep // 128
    run = rec_rows // owners
    for owner in range(owners):
        for r in range(rep):
            start = (owner * rep + r) * run
            tiles[r, pl.ds(owner * run, run), :] = part[start : start + run]
    for r in range(rep):
        at = pl.multiple_of(r * share + group * piece, piece)
        tiles[r, pl.ds(rec_rows, piece), :] = turned[pl.ds(at, piece), :]


def product(normed, rec_cot, conv_out, gate_cot, rep):
    tokens, width = normed.shape
    block = rec_cot.shape[1]
    rows = (width + block) // rep
    fixed = pl.BlockSpec((tokens, block), lambda g: (0, 0))
    flops = 2 * tokens * block * (width + block)
    return pl.pallas_call(
        product_kernel,
        grid=(GROUPS,),
        in_specs=[
            pl.BlockSpec((tokens, width // GROUPS), lambda g: (0, g)),
            fixed,
            fixed,
            fixed,
        ],
        out_specs=pl.BlockSpec((rep, rows // GROUPS, block), lambda g: (0, g, 0)),
        out_shape=jax.ShapeDtypeStruct((rep, rows, block), F32),
        scratch_shapes=[pltpu.VMEM((block, block), F32)],
        cost_estimate=pl.CostEstimate(
            flops=flops, bytes_accessed=1 << 22, transcendentals=0
        ),
    )(normed, rec_cot, conv_out, gate_cot)


def gather_kernel(arrived, tiles, turned):
    rep = arrived.shape[0]
    fs, run, _ = tiles.shape
    rows = arrived.shape[1] // GROUPS
    piece = turned.shape[0] // GROUPS
    owners = fs // GROUPS
    for g in range(GROUPS):
        total = arrived[0, pl.ds(g * rows, rows), :]
        for r in range(1, rep):
            total += arrived[r, pl.ds(g * rows, rows), :]
        for owner in range(owners):
            tiles[g * owners + owner] = total[owner * run : (owner + 1) * run]
        turned[pl.ds(g * piece, piece), :] = total[owners * run :]


def gather(arrived, fs):
    rep, rows, block = arrived.shape
    share = block // rep
    tiles = jax.ShapeDtypeStruct((fs, (rows - share) // fs, block), F32)
    turned = jax.ShapeDtypeStruct((share, block), F32)
    return on_core(gather_kernel, (tiles, turned), (arrived,))


def middle_kernel(rec_tiles, gates, left, tiles):
    fs, run, block = rec_tiles.shape
    half = block // 2
    depth = left.shape[1] // 2
    turned = gates[...]
    blank = jnp.zeros_like(turned)
    done = None
    for q in range(2):
        rows_q = left[:, pl.ds(q * depth, depth), :].reshape(fs * depth, block)
        wide = [blank] * q + [turned]
        wide += [blank] * (half // turned.shape[0] - len(wide))
        term = lax.dot_general(
            rows_q,
            jnp.concatenate(wide, axis=0),
            ALONG_COLUMNS,
            precision=HIGH,
            preferred_element_type=F32,
        )
        done = term if done is None else done + term
    for f in range(fs):
        row, side = f // 2 * depth, f % 2 * half
        tiles[f, pl.ds(0, run), :] = rec_tiles[f]
        tiles[f, pl.ds(run, depth), pl.ds(0, half)] = turned[
            row : row + depth, side : side + half
        ]
        tiles[f, pl.ds(run, depth), pl.ds(half, half)] = done[
            f * depth : (f + 1) * depth
        ]


def middle(rec_tiles, gates, left):
    fs, run, block = rec_tiles.shape
    out = jax.ShapeDtypeStruct((fs, run + left.shape[1] // 2, block), F32)
    return on_core(middle_kernel, (out,), (rec_tiles, gates, left), flops=1 << 30)


def fold_kernel(tiles, copies):
    total = tiles[0]
    for i in range(1, tiles.shape[0]):
        total += tiles[i]
    for i in range(copies.shape[0]):
        copies[i] = total


def fold(tiles, count):
    out = jax.ShapeDtypeStruct((count, *tiles.shape[1:]), F32)
    return on_core(fold_kernel, (out,), (tiles,))


def decay_kernel(rec_moment, gate_moment, rec_out, gate_out):
    rec_out[...] = BETA * rec_moment[...]
    gate_out[...] = BETA * gate_moment[...]


def square_sum(value):
    return jnp.sum(jnp.sum(value * value, axis=0, keepdims=True), axis=1, keepdims=True)


def moments_kernel(
    full,
    rec_right,
    gate_right,
    rec_moment,
    gate_moment,
    rec_out,
    gate_out,
    sums,
):
    rep, _, block = full.shape
    n_rec = rec_moment.shape[0] // rep
    half, share = block // 2, block // rep
    depth = full.shape[1] - n_rec
    rec_grad = full[:, pl.ds(0, n_rec), :].reshape(rep * n_rec, block)
    rec_pre = jnp.dot(
        rec_grad, rec_right[...].astype(F32), precision=HIGH, preferred_element_type=F32
    )
    rec_new = rec_moment[...] + rec_pre
    rec_out[...] = rec_new

    gate_grad = full[:, pl.ds(n_rec, depth), pl.ds(0, half)]
    done = jnp.concatenate(
        [full[r, pl.ds(n_rec, depth), pl.ds(half, half)] for r in range(rep)], axis=1
    )
    right = gate_right[...].astype(F32)
    blank = jnp.zeros((share, block), F32)
    parts = []
    for q in range(2):
        wide = []
        for r in range(rep):
            mine = right[r * share : (r + 1) * share]
            wide += [blank] * q + [mine] + [blank] * (1 - q)
        parts.append(
            jnp.dot(
                done,
                jnp.concatenate(wide, axis=0),
                precision=HIGH,
                preferred_element_type=F32,
            )
        )
    gate_new = gate_moment[...] + jnp.concatenate(parts, axis=0)
    gate_out[...] = gate_new

    row = lax.broadcasted_iota(jnp.int32, sums.shape[1:], 0)
    tile = jnp.zeros(sums.shape[1:], F32)
    squares = (
        square_sum(rec_grad),
        square_sum(rec_new),
        square_sum(gate_grad.reshape(rep * depth, half)),
        square_sum(gate_new),
    )
    for i, value in enumerate(squares):
        tile = jnp.where(row == i, value, tile)
    for i in range(sums.shape[0]):
        sums[i] = tile


def update_kernel(
    sums,
    rec_weight,
    rec_moment,
    gate_weight,
    gate_moment,
    rec_new,
    rec_step,
    rec_copy,
    gate_new,
    gate_step,
    gate_copy,
):
    total = sums[0]
    for i in range(1, sums.shape[0]):
        total += sums[i]
    places = (
        (rec_weight, rec_moment, rec_new, rec_step, rec_copy),
        (gate_weight, gate_moment, gate_new, gate_step, gate_copy),
    )
    for i, (weight, moment, new, step, copy) in enumerate(places):
        scale = jnp.sqrt(total[2 * i : 2 * i + 1]) / jnp.sqrt(
            total[2 * i + 1 : 2 * i + 2] + EPSILON
        )
        scale = jnp.concatenate([LEARN_RATE * scale] * 2, axis=1)
        taken = scale * moment[...]
        value = weight[...] - taken
        step[...] = taken
        new[...] = value
        copy[...] = value.astype(jnp.bfloat16)


def shards(
    normed,
    rec_cot,
    conv_out,
    gate_cot,
    rec_weight,
    rec_moment,
    rec_right,
    gate_weight,
    gate_moment,
    gate_left,
    gate_right,
):
    fs, rep = lax.axis_size("fs"), lax.axis_size("rep")
    like = lambda value, kind=F32: jax.ShapeDtypeStruct(value.shape, kind)
    gate_weight, gate_moment = gate_weight[0], gate_moment[0]

    with jax.named_scope("left"):
        left = gate_left[0].astype(F32)
        left = lax.all_gather(left, "fs")
    with jax.named_scope("product"):
        tiles = product(normed, rec_cot, conv_out, gate_cot, rep)
    with jax.named_scope("near"):
        arrived = exchange(tiles, "rep")
    with jax.named_scope("decay"):
        rec_moment, gate_moment = on_core(
            decay_kernel,
            (like(rec_moment), like(gate_moment)),
            (rec_moment, gate_moment),
        )
    with jax.named_scope("gather"):
        rec_tiles, gates = gather(arrived, fs)
    with jax.named_scope("middle"):
        tiles = middle(rec_tiles, gates, left)
    with jax.named_scope("far"):
        arrived = exchange(tiles, "fs")
    with jax.named_scope("fold"):
        tiles = fold(arrived, rep)
    with jax.named_scope("share"):
        full = exchange(tiles, "rep")
    with jax.named_scope("moments"):
        rec_moment_new, gate_moment_new, sums = on_core(
            moments_kernel,
            (
                like(rec_moment),
                like(gate_moment),
                jax.ShapeDtypeStruct((fs, 8, 128), F32),
            ),
            (full, rec_right, gate_right[0], rec_moment, gate_moment),
        )
    with jax.named_scope("sums"):
        sums = fold(exchange(sums, "fs"), size_of(TP))
        sums = exchange(sums, TP)
    with jax.named_scope("update"):
        bf16 = jnp.bfloat16
        rec_new, rec_step, rec_copy, gate_new, gate_step, gate_copy = on_core(
            update_kernel,
            (
                like(rec_weight),
                like(rec_weight),
                like(rec_weight, bf16),
                like(gate_weight),
                like(gate_weight),
                like(gate_weight, bf16),
            ),
            (sums, rec_weight, rec_moment_new, gate_weight, gate_moment_new),
        )
    return (
        rec_new,
        rec_moment_new,
        rec_step,
        rec_copy,
        gate_new[None],
        gate_moment_new[None],
        gate_step[None],
        gate_copy[None],
    )


def solution(mesh):
    fs, rep, tp = (mesh.shape[name] for name in ("fs", "rep", "tp"))
    split = Mesh(
        mesh.devices.reshape(fs, rep, tp // 2, 2),
        ("fs", "rep", *TP),
    )
    tokens = ("fs", "rep")
    placed = (
        P(tokens, None),
        P(tokens, TP),
        P(tokens, TP),
        P(tokens, TP),
        P("fs", TP),
        P("fs", TP),
        P(TP, None),
        P(TP, "fs", None),
        P(TP, "fs", None),
        P(TP, "fs", None),
        P(TP, None, None),
    )

    return jax.shard_map(
        shards,
        mesh=split,
        in_specs=placed,
        out_specs=(P("fs", TP),) * 4 + (P(TP, "fs", None),) * 4,
        check_vma=False,
    )
```

```python
import jax
import jax.numpy as jnp
from jax import lax
from jax.experimental import pallas as pl
from jax.experimental.pallas import tpu as pltpu
from jax.sharding import Mesh
from jax.sharding import PartitionSpec as P

FS = ("fs_hi", "fs_lo")
TP = ("tp_0", "tp_1")

BETA = 0.9
LEARN_RATE = 0.02
EPSILON = 1e-06
GROUPS = 4
GRANT = 16 << 20
F32 = jnp.float32
HIGH = lax.Precision.HIGHEST
ALONG_ROWS = (((0,), (0,)), ((), ()))
ALONG_COLUMNS = (((1,), (1,)), ((), ()))


def size_of(axes):
    axes = (axes,) if isinstance(axes, str) else axes
    size = 1
    for axis in axes:
        size *= lax.axis_size(axis)
    return size


def exchange(tiles, axes):
    return lax.all_to_all(tiles, axes, split_axis=0, concat_axis=0, tiled=True)


def whole():
    return pl.BlockSpec(memory_space=pltpu.VMEM)


def on_core(kernel, outs, args, scratch=(), flops=1 << 26):
    moved = sum(a.size * a.dtype.itemsize for a in (*args, *outs))
    single = len(outs) == 1
    return pl.pallas_call(
        kernel,
        out_shape=outs[0] if single else outs,
        in_specs=[whole() for _ in args],
        out_specs=whole() if single else [whole() for _ in outs],
        scratch_shapes=list(scratch),
        compiler_params=pltpu.CompilerParams(vmem_limit_bytes=GRANT),
        cost_estimate=pl.CostEstimate(
            flops=flops, bytes_accessed=moved, transcendentals=0
        ),
    )(*args)


def product_kernel(normed, rec_cot, conv_out, gate_cot, right, tiles, turned):
    rep, rows, _ = tiles.shape
    group = pl.program_id(0)

    @pl.when(group == 0)
    def _():
        grad = lax.dot_general(
            gate_cot[...], conv_out[...], ALONG_ROWS, preferred_element_type=F32
        )
        turned[0] = grad
        turned[1] = lax.dot_general(
            right[...].astype(F32),
            grad,
            ALONG_ROWS,
            precision=HIGH,
            preferred_element_type=F32,
        )

    part = lax.dot_general(
        normed[...], rec_cot[...], ALONG_ROWS, preferred_element_type=F32
    )
    share = turned.shape[1] // rep
    piece = share // GROUPS
    rec_rows = rows - 2 * piece
    run = 128 // rep
    for owner in range(rec_rows // run):
        for r in range(rep):
            start = (owner * rep + r) * run
            tiles[r, pl.ds(owner * run, run), :] = part[start : start + run]
    for r in range(rep):
        at = pl.multiple_of(r * share + group * piece, piece)
        for i in range(2):
            tiles[r, pl.ds(rec_rows + i * piece, piece), :] = turned[
                i, pl.ds(at, piece), :
            ]


def product(normed, rec_cot, conv_out, gate_cot, right, rep):
    tokens, width = normed.shape
    block = rec_cot.shape[1]
    rows = (width + 2 * block) // rep
    fixed = pl.BlockSpec((tokens, block), lambda g: (0, 0))
    flops = 2 * tokens * block * (width + block)
    return pl.pallas_call(
        product_kernel,
        grid=(GROUPS,),
        in_specs=[
            pl.BlockSpec((tokens, width // GROUPS), lambda g: (0, g)),
            fixed,
            fixed,
            fixed,
            pl.BlockSpec((block, block), lambda g: (0, 0)),
        ],
        out_specs=pl.BlockSpec((rep, rows // GROUPS, block), lambda g: (0, g, 0)),
        out_shape=jax.ShapeDtypeStruct((rep, rows, block), F32),
        scratch_shapes=[pltpu.VMEM((2, block, block), F32)],
        cost_estimate=pl.CostEstimate(
            flops=flops, bytes_accessed=1 << 22, transcendentals=0
        ),
    )(normed, rec_cot, conv_out, gate_cot, right)


def middle_kernel(arrived, left, tiles):
    rep = arrived.shape[0]
    fs, _, block = tiles.shape
    rows = arrived.shape[1] // GROUPS
    share = block // rep
    piece = share // GROUPS
    rec_rows = rows - 2 * piece
    owners = fs // GROUPS
    run = rec_rows // owners
    half = block // 2
    grads, rights = [], []
    for g in range(GROUPS):
        total = arrived[0, pl.ds(g * rows, rows), :]
        for r in range(1, rep):
            total += arrived[r, pl.ds(g * rows, rows), :]
        for owner in range(owners):
            tiles[g * owners + owner, pl.ds(0, run), :] = total[
                owner * run : (owner + 1) * run
            ]
        grads.append(total[rec_rows : rec_rows + piece])
        rights.append(total[rec_rows + piece :])
    turned = jnp.concatenate(grads, axis=0)
    right_done = jnp.concatenate(rights, axis=0)
    blank = jnp.zeros_like(right_done)
    depth = left.shape[1] // 2
    done = None
    for q in range(2):
        rows_q = left[:, pl.ds(q * depth, depth), :].reshape(fs * depth, block)
        wide = [blank] * q + [right_done] + [blank] * (1 - q)
        term = lax.dot_general(
            rows_q,
            jnp.concatenate(wide, axis=0),
            ALONG_COLUMNS,
            precision=HIGH,
            preferred_element_type=F32,
        )
        done = term if done is None else done + term
    for f in range(fs):
        row, side = f // 2 * depth, f % 2 * half
        tiles[f, pl.ds(run, depth), pl.ds(0, half)] = turned[
            row : row + depth, side : side + half
        ]
        tiles[f, pl.ds(run, depth), pl.ds(half, half)] = done[
            f * depth : (f + 1) * depth
        ]


def middle(arrived, left):
    fs, own_rows, block = left.shape
    rec_rows = arrived.shape[1] - 2 * block // arrived.shape[0]
    out = jax.ShapeDtypeStruct((fs, rec_rows // fs + own_rows // 2, block), F32)
    return on_core(middle_kernel, (out,), (arrived, left), flops=1 << 30)


def fold_kernel(tiles, after, copies):
    total = tiles[0]
    for i in range(1, tiles.shape[0]):
        total += tiles[i]
    for i in range(copies.shape[0]):
        copies[i] = total


def fold(tiles, count, after):
    out = jax.ShapeDtypeStruct((count, *tiles.shape[1:]), F32)
    return on_core(fold_kernel, (out,), (tiles, after))


def square_sum(value):
    return jnp.sum(jnp.sum(value * value, axis=0, keepdims=True), axis=1, keepdims=True)


def placing(block, share, q, r):
    lane = lax.broadcasted_iota(jnp.int32, (2 * share, block), 0) - q * share
    column = lax.broadcasted_iota(jnp.int32, (2 * share, block), 1) - r * share
    inside = (lane >= 0) & (lane < share)
    return jnp.where(inside & (lane == column), 1.0, 0.0).astype(F32)


def settle_kernel(arrived, rec_right, rec_moment, gate_moment, mine, sums):
    _, rows, block = arrived.shape
    rep = lax.axis_size("rep")
    r = lax.axis_index("rep")
    run = rec_moment.shape[0] // rep
    depth = rows - run
    half, share = block // 2, block // rep
    total = arrived[0]
    for i in range(1, arrived.shape[0]):
        total += arrived[i]
    rec_grad = total[:run]
    rec_pre = jnp.dot(
        rec_grad, rec_right[...].astype(F32), precision=HIGH, preferred_element_type=F32
    )
    start = pl.multiple_of(r * run, run)
    rec_new = BETA * rec_moment[pl.ds(start, run), :] + rec_pre
    mine[pl.ds(0, run), :] = rec_new

    gate_grad = total[run:, :half]
    packed = None
    for q in range(2):
        term = lax.dot_general(
            gate_moment[pl.ds(q * depth, depth), :],
            placing(block, share, q, r),
            ALONG_COLUMNS,
            precision=HIGH,
            preferred_element_type=F32,
        )
        packed = term if packed is None else packed + term
    gate_new = BETA * packed + total[run:, half:]
    mine[pl.ds(run, depth), pl.ds(0, half)] = gate_new
    mine[pl.ds(run, depth), pl.ds(half, half)] = gate_new

    row = lax.broadcasted_iota(jnp.int32, sums.shape[1:], 0)
    tile = jnp.zeros(sums.shape[1:], F32)
    for i, value in enumerate((rec_grad, rec_new, gate_grad, gate_new)):
        tile = jnp.where(row == i, square_sum(value), tile)
    for i in range(sums.shape[0]):
        sums[i] = tile


def update_kernel(
    sums,
    full,
    rec_weight,
    gate_weight,
    rec_new,
    rec_moment,
    rec_step,
    rec_copy,
    gate_new,
    gate_moment,
    gate_step,
    gate_copy,
):
    rep, rows, block = full.shape
    run = rec_weight.shape[0] // rep
    depth = rows - run
    half, share = block // 2, block // rep
    rec_value = full[:, pl.ds(0, run), :].reshape(rep * run, block)
    parts = []
    for q in range(2):
        part = None
        for r in range(rep):
            term = jnp.dot(
                full[r, pl.ds(run, depth), pl.ds(0, half)],
                placing(block, share, q, r),
                precision=HIGH,
                preferred_element_type=F32,
            )
            part = term if part is None else part + term
        parts.append(part)
    gate_value = jnp.concatenate(parts, axis=0)

    total = sums[0]
    for i in range(1, sums.shape[0]):
        total += sums[i]
    places = (
        (rec_value, rec_weight, rec_new, rec_moment, rec_step, rec_copy),
        (gate_value, gate_weight, gate_new, gate_moment, gate_step, gate_copy),
    )
    for i, (value, weight, new, moment, step, copy) in enumerate(places):
        scale = jnp.sqrt(total[2 * i : 2 * i + 1]) / jnp.sqrt(
            total[2 * i + 1 : 2 * i + 2] + EPSILON
        )
        scale = jnp.concatenate([LEARN_RATE * scale] * 2, axis=1)
        taken = scale * value
        result = weight[...] - taken
        moment[...] = value
        step[...] = taken
        new[...] = result
        copy[...] = result.astype(jnp.bfloat16)


def shards(
    normed,
    rec_cot,
    conv_out,
    gate_cot,
    rec_weight,
    rec_moment,
    rec_right,
    gate_weight,
    gate_moment,
    gate_left,
    gate_right,
):
    fs, rep = size_of(FS), lax.axis_size("rep")
    like = lambda value, kind=F32: jax.ShapeDtypeStruct(value.shape, kind)
    gate_weight, gate_moment = gate_weight[0], gate_moment[0]
    own_rows, block = gate_weight.shape

    with jax.named_scope("product"):
        tiles = product(normed, rec_cot, conv_out, gate_cot, gate_right[0], rep)
    with jax.named_scope("near"):
        arrived = exchange(tiles, "rep")
    with jax.named_scope("left"):
        left = lax.all_gather(gate_left[0].astype(F32), "fs_lo")
        left = lax.all_gather(left, "fs_hi").reshape(fs, own_rows, block)
    with jax.named_scope("middle"):
        tiles = middle(arrived, left)
    with jax.named_scope("far"):
        arrived = exchange(tiles, FS)
    with jax.named_scope("settle"):
        mine, sums = on_core(
            settle_kernel,
            (
                jax.ShapeDtypeStruct(arrived.shape[1:], F32),
                jax.ShapeDtypeStruct((fs, 8, 128), F32),
            ),
            (arrived, rec_right, rec_moment, gate_moment),
        )
    with jax.named_scope("share"):
        full = lax.all_gather(mine, "rep")
    with jax.named_scope("sums"):
        sums = fold(exchange(sums, FS), rep * size_of(TP), full)
        sums = exchange(sums, ("rep", *TP))
    with jax.named_scope("update"):
        bf16 = jnp.bfloat16
        (
            rec_new,
            rec_moment_new,
            rec_step,
            rec_copy,
            gate_new,
            gate_moment_new,
            gate_step,
            gate_copy,
        ) = on_core(
            update_kernel,
            (
                like(rec_weight),
                like(rec_weight),
                like(rec_weight),
                like(rec_weight, bf16),
                like(gate_weight),
                like(gate_weight),
                like(gate_weight),
                like(gate_weight, bf16),
            ),
            (sums, full, rec_weight, gate_weight),
        )
    return (
        rec_new,
        rec_moment_new,
        rec_step,
        rec_copy,
        gate_new[None],
        gate_moment_new[None],
        gate_step[None],
        gate_copy[None],
    )


def solution(mesh):
    fs, rep, tp = (mesh.shape[name] for name in ("fs", "rep", "tp"))
    split = Mesh(
        mesh.devices.reshape(fs // 4, 4, rep, tp // 2, 2),
        (*FS, "rep", *TP),
    )
    tokens = (*FS, "rep")
    placed = (
        P(tokens, None),
        P(tokens, TP),
        P(tokens, TP),
        P(tokens, TP),
        P(FS, TP),
        P(FS, TP),
        P(TP, None),
        P(TP, FS, None),
        P(TP, FS, None),
        P(TP, FS, None),
        P(TP, None, None),
    )

    return jax.shard_map(
        shards,
        mesh=split,
        in_specs=placed,
        out_specs=(P(FS, TP),) * 4 + (P(TP, FS, None),) * 4,
        check_vma=False,
    )
```

```python
import jax
import jax.numpy as jnp
from jax import lax
from jax.experimental import pallas as pl
from jax.experimental.pallas import tpu as pltpu
from jax.sharding import Mesh
from jax.sharding import PartitionSpec as P

TP = ("tp_0", "tp_1")

BETA = 0.9
LEARN_RATE = 0.02
EPSILON = 1e-06
GROUPS = 4
GRANT = 16 << 20
F32 = jnp.float32
HIGH = lax.Precision.HIGHEST
ALONG_ROWS = (((0,), (0,)), ((), ()))
ALONG_COLUMNS = (((1,), (1,)), ((), ()))


def size_of(axes):
    axes = (axes,) if isinstance(axes, str) else axes
    size = 1
    for axis in axes:
        size *= lax.axis_size(axis)
    return size


def exchange(tiles, axes):
    return lax.all_to_all(tiles, axes, split_axis=0, concat_axis=0, tiled=True)


def whole():
    return pl.BlockSpec(memory_space=pltpu.VMEM)


def on_core(kernel, outs, args, scratch=(), flops=1 << 26):
    moved = sum(a.size * a.dtype.itemsize for a in (*args, *outs))
    single = len(outs) == 1
    return pl.pallas_call(
        kernel,
        out_shape=outs[0] if single else outs,
        in_specs=[whole() for _ in args],
        out_specs=whole() if single else [whole() for _ in outs],
        scratch_shapes=list(scratch),
        compiler_params=pltpu.CompilerParams(vmem_limit_bytes=GRANT),
        cost_estimate=pl.CostEstimate(
            flops=flops, bytes_accessed=moved, transcendentals=0
        ),
    )(*args)


def product_kernel(
    normed, rec_cot, conv_hbm, cot_hbm, right_hbm, tiles, conv_out, gate_cot, right, sems
):
    rep, rows, block = tiles.shape
    group = pl.program_id(0)
    copies = [
        pltpu.make_async_copy(source, target, sems.at[i])
        for i, (source, target) in enumerate(
            ((conv_hbm, conv_out), (cot_hbm, gate_cot), (right_hbm, right))
        )
    ]

    @pl.when(group == 0)
    def _():
        for copy in copies:
            copy.start()

    @pl.when(group < GROUPS)
    def _():
        part = lax.dot_general(
            normed[...], rec_cot[...], ALONG_ROWS, preferred_element_type=F32
        )
        run = 128 // rep
        for owner in range(rows // run):
            for r in range(rep):
                start = (owner * rep + r) * run
                tiles[r, pl.ds(owner * run, run), :] = part[start : start + run]

    @pl.when(group == GROUPS)
    def _():
        for copy in copies:
            copy.wait()
        grad = lax.dot_general(
            gate_cot[...], conv_out[...], ALONG_ROWS, preferred_element_type=F32
        )
        done = lax.dot_general(
            right[...].astype(F32),
            grad,
            ALONG_ROWS,
            precision=HIGH,
            preferred_element_type=F32,
        )
        share = block // rep
        for r in range(rep):
            for i, value in enumerate((grad, done)):
                tiles[r, pl.ds(i * share, share), :] = value[
                    r * share : (r + 1) * share
                ]


def product(normed, rec_cot, conv_out, gate_cot, right, rep):
    tokens, width = normed.shape
    block = rec_cot.shape[1]
    rows = width // GROUPS // rep
    flops = 2 * tokens * block * (width + block)
    held = lambda value: pltpu.VMEM(value.shape, value.dtype)
    return pl.pallas_call(
        product_kernel,
        grid=(GROUPS + 1,),
        in_specs=[
            pl.BlockSpec(
                (tokens, width // GROUPS), lambda g: (0, jnp.minimum(g, GROUPS - 1))
            ),
            pl.BlockSpec((tokens, block), lambda g: (0, 0)),
            *[pl.BlockSpec(memory_space=pl.ANY)] * 3,
        ],
        out_specs=pl.BlockSpec((rep, rows, block), lambda g: (0, g, 0)),
        out_shape=jax.ShapeDtypeStruct((rep, rows * (GROUPS + 1), block), F32),
        scratch_shapes=[
            held(conv_out),
            held(gate_cot),
            held(right),
            pltpu.SemaphoreType.DMA((3,)),
        ],
        cost_estimate=pl.CostEstimate(
            flops=flops, bytes_accessed=1 << 22, transcendentals=0
        ),
    )(normed, rec_cot, conv_out, gate_cot, right)


def middle_kernel(arrived, left, tiles):
    rep = arrived.shape[0]
    fs, _, block = tiles.shape
    half, share = block // 2, block // rep
    rec_rows = arrived.shape[1] - 2 * share
    run = rec_rows // fs

    def total(start, size):
        value = arrived[0, pl.ds(start, size), :]
        for r in range(1, rep):
            value += arrived[r, pl.ds(start, size), :]
        return value

    for f in range(fs):
        tiles[f, pl.ds(0, run), :] = total(f * run, run)
    turned = total(rec_rows, share)
    right_done = total(rec_rows + share, share)
    blank = jnp.zeros_like(right_done)
    depth = left.shape[1] // 2
    done = None
    for q in range(2):
        rows_q = left[:, pl.ds(q * depth, depth), :].reshape(fs * depth, block)
        wide = [blank] * q + [right_done] + [blank] * (1 - q)
        term = lax.dot_general(
            rows_q,
            jnp.concatenate(wide, axis=0),
            ALONG_COLUMNS,
            precision=HIGH,
            preferred_element_type=F32,
        )
        done = term if done is None else done + term
    for f in range(fs):
        row, side = f // 2 * depth, f % 2 * half
        tiles[f, pl.ds(run, depth), pl.ds(0, half)] = turned[
            row : row + depth, side : side + half
        ]
        tiles[f, pl.ds(run, depth), pl.ds(half, half)] = done[
            f * depth : (f + 1) * depth
        ]


def middle(arrived, left):
    fs, own_rows, block = left.shape
    rec_rows = arrived.shape[1] - 2 * block // arrived.shape[0]
    out = jax.ShapeDtypeStruct((fs, rec_rows // fs + own_rows // 2, block), F32)
    return on_core(middle_kernel, (out,), (arrived, left), flops=1 << 30)


def fold_kernel(tiles, after, copies):
    total = tiles[0]
    for i in range(1, tiles.shape[0]):
        total += tiles[i]
    for i in range(copies.shape[0]):
        copies[i] = total


def fold(tiles, count, after):
    out = jax.ShapeDtypeStruct((count, *tiles.shape[1:]), F32)
    return on_core(fold_kernel, (out,), (tiles, after))


def square_sum(value):
    return jnp.sum(jnp.sum(value * value, axis=0, keepdims=True), axis=1, keepdims=True)


def placing(block, share, q, r):
    lane = lax.broadcasted_iota(jnp.int32, (2 * share, block), 0) - q * share
    column = lax.broadcasted_iota(jnp.int32, (2 * share, block), 1) - r * share
    inside = (lane >= 0) & (lane < share)
    return jnp.where(inside & (lane == column), 1.0, 0.0).astype(F32)


def settle_kernel(arrived, rec_right, rec_moment, gate_moment, mine, sums):
    _, rows, block = arrived.shape
    rep = lax.axis_size("rep")
    r = lax.axis_index("rep")
    run = rec_moment.shape[0] // rep
    depth = rows - run
    half, share = block // 2, block // rep
    total = arrived[0]
    for i in range(1, arrived.shape[0]):
        total += arrived[i]
    rec_grad = total[:run]
    rec_pre = jnp.dot(
        rec_grad, rec_right[...].astype(F32), precision=HIGH, preferred_element_type=F32
    )
    start = pl.multiple_of(r * run, run)
    rec_new = BETA * rec_moment[pl.ds(start, run), :] + rec_pre
    mine[pl.ds(0, run), :] = rec_new

    gate_grad = total[run:, :half]
    packed = None
    for q in range(2):
        term = lax.dot_general(
            gate_moment[pl.ds(q * depth, depth), :],
            placing(block, share, q, r),
            ALONG_COLUMNS,
            precision=HIGH,
            preferred_element_type=F32,
        )
        packed = term if packed is None else packed + term
    gate_new = BETA * packed + total[run:, half:]
    mine[pl.ds(run, depth), pl.ds(0, half)] = gate_new
    mine[pl.ds(run, depth), pl.ds(half, half)] = gate_new

    row = lax.broadcasted_iota(jnp.int32, sums.shape[1:], 0)
    tile = jnp.zeros(sums.shape[1:], F32)
    for i, value in enumerate((rec_grad, rec_new, gate_grad, gate_new)):
        tile = jnp.where(row == i, square_sum(value), tile)
    for i in range(sums.shape[0]):
        sums[i] = tile


def update_kernel(
    sums,
    full,
    rec_weight,
    gate_weight,
    rec_new,
    rec_moment,
    rec_step,
    rec_copy,
    gate_new,
    gate_moment,
    gate_step,
    gate_copy,
):
    rep, rows, block = full.shape
    run = rec_weight.shape[0] // rep
    depth = rows - run
    half, share = block // 2, block // rep
    rec_value = full[:, pl.ds(0, run), :].reshape(rep * run, block)
    parts = []
    for q in range(2):
        part = None
        for r in range(rep):
            term = jnp.dot(
                full[r, pl.ds(run, depth), pl.ds(0, half)],
                placing(block, share, q, r),
                precision=HIGH,
                preferred_element_type=F32,
            )
            part = term if part is None else part + term
        parts.append(part)
    gate_value = jnp.concatenate(parts, axis=0)

    total = sums[0]
    for i in range(1, sums.shape[0]):
        total += sums[i]
    places = (
        (rec_value, rec_weight, rec_new, rec_moment, rec_step, rec_copy),
        (gate_value, gate_weight, gate_new, gate_moment, gate_step, gate_copy),
    )
    for i, (value, weight, new, moment, step, copy) in enumerate(places):
        scale = jnp.sqrt(total[2 * i : 2 * i + 1]) / jnp.sqrt(
            total[2 * i + 1 : 2 * i + 2] + EPSILON
        )
        scale = jnp.concatenate([LEARN_RATE * scale] * 2, axis=1)
        taken = scale * value
        result = weight[...] - taken
        moment[...] = value
        step[...] = taken
        new[...] = result
        copy[...] = result.astype(jnp.bfloat16)


def shards(
    normed,
    rec_cot,
    conv_out,
    gate_cot,
    rec_weight,
    rec_moment,
    rec_right,
    gate_weight,
    gate_moment,
    gate_left,
    gate_right,
):
    fs, rep = lax.axis_size("fs"), lax.axis_size("rep")
    like = lambda value, kind=F32: jax.ShapeDtypeStruct(value.shape, kind)
    gate_weight, gate_moment = gate_weight[0], gate_moment[0]

    with jax.named_scope("product"):
        tiles = product(normed, rec_cot, conv_out, gate_cot, gate_right[0], rep)
    with jax.named_scope("near"):
        arrived = exchange(tiles, "rep")
    with jax.named_scope("left"):
        left = lax.all_gather(gate_left[0].astype(F32), "fs", tiled=True).reshape(fs, *gate_left.shape[1:])
    with jax.named_scope("middle"):
        tiles = middle(arrived, left)
    with jax.named_scope("far"):
        arrived = exchange(tiles, "fs")
    with jax.named_scope("settle"):
        mine, sums = on_core(
            settle_kernel,
            (
                jax.ShapeDtypeStruct(arrived.shape[1:], F32),
                jax.ShapeDtypeStruct((fs, 4, 128), F32),
            ),
            (arrived, rec_right, rec_moment, gate_moment),
        )
    with jax.named_scope("share"):
        full = lax.all_gather(mine, "rep")
    with jax.named_scope("sums"):
        sums = fold(exchange(sums, "fs"), rep * size_of(TP), full)
        sums = exchange(sums, ("rep", *TP))
    with jax.named_scope("update"):
        bf16 = jnp.bfloat16
        (
            rec_new,
            rec_moment_new,
            rec_step,
            rec_copy,
            gate_new,
            gate_moment_new,
            gate_step,
            gate_copy,
        ) = on_core(
            update_kernel,
            (
                like(rec_weight),
                like(rec_weight),
                like(rec_weight),
                like(rec_weight, bf16),
                like(gate_weight),
                like(gate_weight),
                like(gate_weight),
                like(gate_weight, bf16),
            ),
            (sums, full, rec_weight, gate_weight),
        )
    return (
        rec_new,
        rec_moment_new,
        rec_step,
        rec_copy,
        gate_new[None],
        gate_moment_new[None],
        gate_step[None],
        gate_copy[None],
    )


def solution(mesh):
    fs, rep, tp = (mesh.shape[name] for name in ("fs", "rep", "tp"))
    split = Mesh(
        mesh.devices.reshape(fs, rep, tp // 2, 2),
        ("fs", "rep", *TP),
    )
    tokens = ("fs", "rep")
    placed = (
        P(tokens, None),
        P(tokens, TP),
        P(tokens, TP),
        P(tokens, TP),
        P("fs", TP),
        P("fs", TP),
        P(TP, None),
        P(TP, "fs", None),
        P(TP, "fs", None),
        P(TP, "fs", None),
        P(TP, None, None),
    )

    return jax.shard_map(
        shards,
        mesh=split,
        in_specs=placed,
        out_specs=(P("fs", TP),) * 4 + (P(TP, "fs", None),) * 4,
        check_vma=False,
    )
```

```python
import jax
import jax.numpy as jnp
from jax import lax
from jax.experimental import pallas as pl
from jax.experimental.pallas import tpu as pltpu
from jax.sharding import Mesh
from jax.sharding import PartitionSpec as P

FS = ("fs_hi", "fs_lo")
TP = ("tp_0", "tp_1")

BETA = 0.9
LEARN_RATE = 0.02
EPSILON = 1e-06
GROUPS = 4
GRANT = 16 << 20
F32 = jnp.float32
HIGH = lax.Precision.HIGHEST
ALONG_ROWS = (((0,), (0,)), ((), ()))
ALONG_COLUMNS = (((1,), (1,)), ((), ()))


def size_of(axes):
    axes = (axes,) if isinstance(axes, str) else axes
    size = 1
    for axis in axes:
        size *= lax.axis_size(axis)
    return size


def exchange(tiles, axes):
    return lax.all_to_all(tiles, axes, split_axis=0, concat_axis=0, tiled=True)


def whole():
    return pl.BlockSpec(memory_space=pltpu.VMEM)


def on_core(kernel, outs, args, scratch=(), flops=1 << 26):
    moved = sum(a.size * a.dtype.itemsize for a in (*args, *outs))
    single = len(outs) == 1
    return pl.pallas_call(
        kernel,
        out_shape=outs[0] if single else outs,
        in_specs=[whole() for _ in args],
        out_specs=whole() if single else [whole() for _ in outs],
        scratch_shapes=list(scratch),
        compiler_params=pltpu.CompilerParams(vmem_limit_bytes=GRANT),
        cost_estimate=pl.CostEstimate(
            flops=flops, bytes_accessed=moved, transcendentals=0
        ),
    )(*args)


def product_kernel(
    normed, rec_cot, conv_hbm, cot_hbm, right_hbm, tiles, conv_out, gate_cot, right, sems
):
    rep, rows, block = tiles.shape
    group = pl.program_id(0)
    copies = [
        pltpu.make_async_copy(source, target, sems.at[i])
        for i, (source, target) in enumerate(
            ((conv_hbm, conv_out), (cot_hbm, gate_cot), (right_hbm, right))
        )
    ]

    @pl.when(group == 0)
    def _():
        for copy in copies:
            copy.start()

    @pl.when(group < GROUPS)
    def _():
        part = lax.dot_general(
            normed[...], rec_cot[...], ALONG_ROWS, preferred_element_type=F32
        )
        run = 128 // rep
        for owner in range(rows // run):
            for r in range(rep):
                start = (owner * rep + r) * run
                tiles[r, pl.ds(owner * run, run), :] = part[start : start + run]

    @pl.when(group == GROUPS)
    def _():
        for copy in copies:
            copy.wait()
        grad = lax.dot_general(
            gate_cot[...], conv_out[...], ALONG_ROWS, preferred_element_type=F32
        )
        done = lax.dot_general(
            right[...].astype(F32),
            grad,
            ALONG_ROWS,
            precision=HIGH,
            preferred_element_type=F32,
        )
        share = block // rep
        for r in range(rep):
            for i, value in enumerate((grad, done)):
                tiles[r, pl.ds(i * share, share), :] = value[
                    r * share : (r + 1) * share
                ]


def product(normed, rec_cot, conv_out, gate_cot, right, rep):
    tokens, width = normed.shape
    block = rec_cot.shape[1]
    rows = width // GROUPS // rep
    flops = 2 * tokens * block * (width + block)
    held = lambda value: pltpu.VMEM(value.shape, value.dtype)
    return pl.pallas_call(
        product_kernel,
        grid=(GROUPS + 1,),
        in_specs=[
            pl.BlockSpec(
                (tokens, width // GROUPS), lambda g: (0, jnp.minimum(g, GROUPS - 1))
            ),
            pl.BlockSpec((tokens, block), lambda g: (0, 0)),
            *[pl.BlockSpec(memory_space=pl.ANY)] * 3,
        ],
        out_specs=pl.BlockSpec((rep, rows, block), lambda g: (0, g, 0)),
        out_shape=jax.ShapeDtypeStruct((rep, rows * (GROUPS + 1), block), F32),
        scratch_shapes=[
            held(conv_out),
            held(gate_cot),
            held(right),
            pltpu.SemaphoreType.DMA((3,)),
        ],
        cost_estimate=pl.CostEstimate(
            flops=flops, bytes_accessed=1 << 22, transcendentals=0
        ),
    )(normed, rec_cot, conv_out, gate_cot, right)


def middle_kernel(arrived, left, tiles):
    rep = arrived.shape[0]
    fs, _, block = tiles.shape
    half, share = block // 2, block // rep
    rec_rows = arrived.shape[1] - 2 * share
    run = rec_rows // fs

    def total(start, size):
        value = arrived[0, pl.ds(start, size), :]
        for r in range(1, rep):
            value += arrived[r, pl.ds(start, size), :]
        return value

    lo = lax.axis_size("fs_lo")
    place = [f % lo * (fs // lo) + f // lo for f in range(fs)]
    for f in range(fs):
        tiles[place[f], pl.ds(0, run), :] = total(f * run, run)
    turned = total(rec_rows, share)
    right_done = total(rec_rows + share, share)
    blank = jnp.zeros_like(right_done)
    depth = left.shape[1] // 2
    done = None
    for q in range(2):
        rows_q = left[:, pl.ds(q * depth, depth), :].reshape(fs * depth, block)
        wide = [blank] * q + [right_done] + [blank] * (1 - q)
        term = lax.dot_general(
            rows_q,
            jnp.concatenate(wide, axis=0),
            ALONG_COLUMNS,
            precision=HIGH,
            preferred_element_type=F32,
        )
        done = term if done is None else done + term
    for f in range(fs):
        row, side = f // 2 * depth, f % 2 * half
        tiles[place[f], pl.ds(run, depth), pl.ds(0, half)] = turned[
            row : row + depth, side : side + half
        ]
        tiles[place[f], pl.ds(run, depth), pl.ds(half, half)] = done[
            f * depth : (f + 1) * depth
        ]


def middle(arrived, left):
    fs, own_rows, block = left.shape
    rec_rows = arrived.shape[1] - 2 * block // arrived.shape[0]
    out = jax.ShapeDtypeStruct((fs, rec_rows // fs + own_rows // 2, block), F32)
    return on_core(middle_kernel, (out,), (arrived, left), flops=1 << 30)


def add_kernel(tiles, total):
    value = tiles[0]
    for i in range(1, tiles.shape[0]):
        value += tiles[i]
    total[...] = value


def add_up(tiles):
    return on_core(
        add_kernel, (jax.ShapeDtypeStruct(tiles.shape[1:], F32),), (tiles,)
    )


def fold_kernel(tiles, after, copies):
    total = tiles[0]
    for i in range(1, tiles.shape[0]):
        total += tiles[i]
    for i in range(copies.shape[0]):
        copies[i] = total


def fold(tiles, count, after):
    out = jax.ShapeDtypeStruct((count, *tiles.shape[1:]), F32)
    return on_core(fold_kernel, (out,), (tiles, after))


def square_sum(value):
    return jnp.sum(jnp.sum(value * value, axis=0, keepdims=True), axis=1, keepdims=True)


def placing(block, share, q, r):
    lane = lax.broadcasted_iota(jnp.int32, (2 * share, block), 0) - q * share
    column = lax.broadcasted_iota(jnp.int32, (2 * share, block), 1) - r * share
    inside = (lane >= 0) & (lane < share)
    return jnp.where(inside & (lane == column), 1.0, 0.0).astype(F32)


def settle_kernel(arrived, rec_right, rec_moment, gate_moment, mine, sums):
    _, rows, block = arrived.shape
    rep = lax.axis_size("rep")
    r = lax.axis_index("rep")
    run = rec_moment.shape[0] // rep
    depth = rows - run
    half, share = block // 2, block // rep
    total = arrived[0]
    for i in range(1, arrived.shape[0]):
        total += arrived[i]
    rec_grad = total[:run]
    rec_pre = jnp.dot(
        rec_grad, rec_right[...].astype(F32), precision=HIGH, preferred_element_type=F32
    )
    start = pl.multiple_of(r * run, run)
    rec_new = BETA * rec_moment[pl.ds(start, run), :] + rec_pre
    mine[pl.ds(0, run), :] = rec_new

    gate_grad = total[run:, :half]
    packed = None
    for q in range(2):
        term = lax.dot_general(
            gate_moment[pl.ds(q * depth, depth), :],
            placing(block, share, q, r),
            ALONG_COLUMNS,
            precision=HIGH,
            preferred_element_type=F32,
        )
        packed = term if packed is None else packed + term
    gate_new = BETA * packed + total[run:, half:]
    mine[pl.ds(run, depth), pl.ds(0, half)] = gate_new
    mine[pl.ds(run, depth), pl.ds(half, half)] = gate_new

    row = lax.broadcasted_iota(jnp.int32, sums.shape[1:], 0)
    tile = jnp.zeros(sums.shape[1:], F32)
    for i, value in enumerate((rec_grad, rec_new, gate_grad, gate_new)):
        tile = jnp.where(row == i, square_sum(value), tile)
    for i in range(sums.shape[0]):
        sums[i] = tile


def update_kernel(
    sums,
    full,
    rec_weight,
    gate_weight,
    rec_new,
    rec_moment,
    rec_step,
    rec_copy,
    gate_new,
    gate_moment,
    gate_step,
    gate_copy,
):
    rep, rows, block = full.shape
    run = rec_weight.shape[0] // rep
    depth = rows - run
    half, share = block // 2, block // rep
    rec_value = full[:, pl.ds(0, run), :].reshape(rep * run, block)
    parts = []
    for q in range(2):
        part = None
        for r in range(rep):
            term = jnp.dot(
                full[r, pl.ds(run, depth), pl.ds(0, half)],
                placing(block, share, q, r),
                precision=HIGH,
                preferred_element_type=F32,
            )
            part = term if part is None else part + term
        parts.append(part)
    gate_value = jnp.concatenate(parts, axis=0)

    total = sums[0]
    for i in range(1, sums.shape[0]):
        total += sums[i]
    places = (
        (rec_value, rec_weight, rec_new, rec_moment, rec_step, rec_copy),
        (gate_value, gate_weight, gate_new, gate_moment, gate_step, gate_copy),
    )
    for i, (value, weight, new, moment, step, copy) in enumerate(places):
        scale = jnp.sqrt(total[2 * i : 2 * i + 1]) / jnp.sqrt(
            total[2 * i + 1 : 2 * i + 2] + EPSILON
        )
        scale = jnp.concatenate([LEARN_RATE * scale] * 2, axis=1)
        taken = scale * value
        result = weight[...] - taken
        moment[...] = value
        step[...] = taken
        new[...] = result
        copy[...] = result.astype(jnp.bfloat16)


def shards(
    normed,
    rec_cot,
    conv_out,
    gate_cot,
    rec_weight,
    rec_moment,
    rec_right,
    gate_weight,
    gate_moment,
    gate_left,
    gate_right,
):
    fs, rep = size_of(FS), lax.axis_size("rep")
    like = lambda value, kind=F32: jax.ShapeDtypeStruct(value.shape, kind)
    gate_weight, gate_moment = gate_weight[0], gate_moment[0]

    with jax.named_scope("product"):
        tiles = product(normed, rec_cot, conv_out, gate_cot, gate_right[0], rep)
    with jax.named_scope("near"):
        arrived = exchange(tiles, "rep")
    with jax.named_scope("left"):
        left = lax.all_gather(gate_left[0].astype(F32), FS, tiled=True).reshape(fs, *gate_left.shape[1:])
    with jax.named_scope("middle"):
        tiles = middle(arrived, left)
    with jax.named_scope("quarter"):
        hi, lo = lax.axis_size("fs_hi"), lax.axis_size("fs_lo")
        rows = tiles.shape[1]
        tiles = add_up(exchange(tiles.reshape(lo, hi * rows, -1), "fs_lo"))
    with jax.named_scope("far"):
        arrived = exchange(tiles.reshape(hi, rows, -1), "fs_hi")
    with jax.named_scope("settle"):
        mine, sums = on_core(
            settle_kernel,
            (
                jax.ShapeDtypeStruct(arrived.shape[1:], F32),
                jax.ShapeDtypeStruct((fs, 4, 128), F32),
            ),
            (arrived, rec_right, rec_moment, gate_moment),
        )
    with jax.named_scope("share"):
        full = lax.all_gather(mine, "rep")
    with jax.named_scope("sums"):
        sums = fold(exchange(sums, FS), rep * size_of(TP), full)
        sums = exchange(sums, ("rep", *TP))
    with jax.named_scope("update"):
        bf16 = jnp.bfloat16
        (
            rec_new,
            rec_moment_new,
            rec_step,
            rec_copy,
            gate_new,
            gate_moment_new,
            gate_step,
            gate_copy,
        ) = on_core(
            update_kernel,
            (
                like(rec_weight),
                like(rec_weight),
                like(rec_weight),
                like(rec_weight, bf16),
                like(gate_weight),
                like(gate_weight),
                like(gate_weight),
                like(gate_weight, bf16),
            ),
            (sums, full, rec_weight, gate_weight),
        )
    return (
        rec_new,
        rec_moment_new,
        rec_step,
        rec_copy,
        gate_new[None],
        gate_moment_new[None],
        gate_step[None],
        gate_copy[None],
    )


def solution(mesh):
    fs, rep, tp = (mesh.shape[name] for name in ("fs", "rep", "tp"))
    split = Mesh(
        mesh.devices.reshape(fs // 4, 4, rep, tp // 2, 2),
        (*FS, "rep", *TP),
    )
    tokens = (*FS, "rep")
    placed = (
        P(tokens, None),
        P(tokens, TP),
        P(tokens, TP),
        P(tokens, TP),
        P(FS, TP),
        P(FS, TP),
        P(TP, None),
        P(TP, FS, None),
        P(TP, FS, None),
        P(TP, FS, None),
        P(TP, None, None),
    )

    return jax.shard_map(
        shards,
        mesh=split,
        in_specs=placed,
        out_specs=(P(FS, TP),) * 4 + (P(TP, FS, None),) * 4,
        check_vma=False,
    )
```

```python
import jax
import jax.numpy as jnp
from jax import lax
from jax.experimental import pallas as pl
from jax.experimental.pallas import tpu as pltpu
from jax.sharding import Mesh
from jax.sharding import PartitionSpec as P

FS = ("fs_hi", "fs_lo")
TP = ("tp_0", "tp_1")

BETA = 0.9
LEARN_RATE = 0.02
EPSILON = 1e-06
PIECES = 4
GRANT = 16 << 20
F32 = jnp.float32
HIGH = lax.Precision.HIGHEST
ALONG_ROWS = (((0,), (0,)), ((), ()))
ALONG_COLUMNS = (((1,), (1,)), ((), ()))


def size_of(axes):
    axes = (axes,) if isinstance(axes, str) else axes
    size = 1
    for axis in axes:
        size *= lax.axis_size(axis)
    return size


def exchange(tiles, axes):
    return lax.all_to_all(tiles, axes, split_axis=0, concat_axis=0, tiled=True)


def whole():
    return pl.BlockSpec(memory_space=pltpu.VMEM)


def on_core(kernel, outs, args, scratch=(), flops=1 << 26):
    moved = sum(a.size * a.dtype.itemsize for a in (*args, *outs))
    single = len(outs) == 1
    return pl.pallas_call(
        kernel,
        out_shape=outs[0] if single else outs,
        in_specs=[whole() for _ in args],
        out_specs=whole() if single else [whole() for _ in outs],
        scratch_shapes=list(scratch),
        compiler_params=pltpu.CompilerParams(vmem_limit_bytes=GRANT),
        cost_estimate=pl.CostEstimate(
            flops=flops, bytes_accessed=moved, transcendentals=0
        ),
    )(*args)


def product_kernel(
    normed_hbm,
    cot_hbm,
    conv_hbm,
    gate_hbm,
    right_hbm,
    tiles_hbm,
    normed,
    rec_cot,
    conv_out,
    gate_cot,
    right,
    tiles,
    in_sems,
    out_sems,
):
    rep, rows, block = tiles.shape
    share = block // rep
    rec_rows = rows - 2 * share
    step = rec_rows // PIECES
    run = 128 // rep

    small = [
        pltpu.make_async_copy(source, target, in_sems.at[i])
        for i, (source, target) in enumerate(
            (
                (conv_hbm, conv_out),
                (gate_hbm, gate_cot),
                (right_hbm, right),
                (cot_hbm, rec_cot),
            )
        )
    ]
    large = pltpu.make_async_copy(normed_hbm, normed, in_sems.at[len(small)])
    for copy in (*small, large):
        copy.start()

    def send(start, size, i):
        part = (slice(None), pl.ds(start, size), slice(None))
        copy = pltpu.make_async_copy(tiles.at[part], tiles_hbm.at[part], out_sems.at[i])
        copy.start()
        return copy

    sent = []
    for copy in small:
        copy.wait()
    grad = lax.dot_general(
        gate_cot[...], conv_out[...], ALONG_ROWS, preferred_element_type=F32
    )
    done = lax.dot_general(
        right[...].astype(F32),
        grad,
        ALONG_ROWS,
        precision=HIGH,
        preferred_element_type=F32,
    )
    for r in range(rep):
        for i, value in enumerate((grad, done)):
            tiles[r, pl.ds(rec_rows + i * share, share), :] = value[
                r * share : (r + 1) * share
            ]
    sent.append(send(rec_rows, 2 * share, PIECES))
    large.wait()
    part = lax.dot_general(
        normed[...], rec_cot[...], ALONG_ROWS, preferred_element_type=F32
    )
    for piece in range(PIECES):
        for owner in range(piece * step // run, (piece + 1) * step // run):
            for r in range(rep):
                start = (owner * rep + r) * run
                tiles[r, pl.ds(owner * run, run), :] = part[start : start + run]
        sent.append(send(piece * step, step, piece))
    for copy in sent:
        copy.wait()


def product(normed, rec_cot, conv_out, gate_cot, right, rep):
    tokens, width = normed.shape
    block = rec_cot.shape[1]
    rows = (width + 2 * block) // rep
    args = (normed, rec_cot, conv_out, gate_cot, right)
    return pl.pallas_call(
        product_kernel,
        in_specs=[pl.BlockSpec(memory_space=pl.ANY)] * len(args),
        out_specs=pl.BlockSpec(memory_space=pl.ANY),
        out_shape=jax.ShapeDtypeStruct((rep, rows, block), F32),
        scratch_shapes=[
            *[pltpu.VMEM(value.shape, value.dtype) for value in args],
            pltpu.VMEM((rep, rows, block), F32),
            pltpu.SemaphoreType.DMA((len(args),)),
            pltpu.SemaphoreType.DMA((PIECES + 1,)),
        ],
        cost_estimate=pl.CostEstimate(
            flops=2 * tokens * block * (width + block),
            bytes_accessed=1 << 22,
            transcendentals=0,
        ),
    )(*args)


def middle_kernel(arrived, left, tiles):
    rep = arrived.shape[0]
    fs, _, block = tiles.shape
    half, share = block // 2, block // rep
    rec_rows = arrived.shape[1] - 2 * share
    run = rec_rows // fs

    def total(start, size):
        value = arrived[0, pl.ds(start, size), :]
        for r in range(1, rep):
            value += arrived[r, pl.ds(start, size), :]
        return value

    lo = lax.axis_size("fs_lo")
    place = [f % lo * (fs // lo) + f // lo for f in range(fs)]
    for f in range(fs):
        tiles[place[f], pl.ds(0, run), :] = total(f * run, run)
    turned = total(rec_rows, share)
    right_done = total(rec_rows + share, share)
    blank = jnp.zeros_like(right_done)
    depth = left.shape[1] // 2
    done = None
    for q in range(2):
        rows_q = left[:, pl.ds(q * depth, depth), :].reshape(fs * depth, block)
        wide = [blank] * q + [right_done] + [blank] * (1 - q)
        term = lax.dot_general(
            rows_q,
            jnp.concatenate(wide, axis=0),
            ALONG_COLUMNS,
            precision=HIGH,
            preferred_element_type=F32,
        )
        done = term if done is None else done + term
    for f in range(fs):
        row, side = f // 2 * depth, f % 2 * half
        tiles[place[f], pl.ds(run, depth), pl.ds(0, half)] = turned[
            row : row + depth, side : side + half
        ]
        tiles[place[f], pl.ds(run, depth), pl.ds(half, half)] = done[
            f * depth : (f + 1) * depth
        ]


def middle(arrived, left):
    fs, own_rows, block = left.shape
    rec_rows = arrived.shape[1] - 2 * block // arrived.shape[0]
    out = jax.ShapeDtypeStruct((fs, rec_rows // fs + own_rows // 2, block), F32)
    return on_core(middle_kernel, (out,), (arrived, left), flops=1 << 30)


def add_kernel(tiles, total):
    value = tiles[0]
    for i in range(1, tiles.shape[0]):
        value += tiles[i]
    total[...] = value


def add_up(tiles):
    return on_core(
        add_kernel, (jax.ShapeDtypeStruct(tiles.shape[1:], F32),), (tiles,)
    )


def fold_kernel(tiles, after, copies):
    total = tiles[0]
    for i in range(1, tiles.shape[0]):
        total += tiles[i]
    for i in range(copies.shape[0]):
        copies[i] = total


def fold(tiles, count, after):
    out = jax.ShapeDtypeStruct((count, *tiles.shape[1:]), F32)
    return on_core(fold_kernel, (out,), (tiles, after))


def square_sum(value):
    return jnp.sum(jnp.sum(value * value, axis=0, keepdims=True), axis=1, keepdims=True)


def placing(block, share, q, r):
    lane = lax.broadcasted_iota(jnp.int32, (2 * share, block), 0) - q * share
    column = lax.broadcasted_iota(jnp.int32, (2 * share, block), 1) - r * share
    inside = (lane >= 0) & (lane < share)
    return jnp.where(inside & (lane == column), 1.0, 0.0).astype(F32)


def settle_kernel(arrived, rec_right, rec_moment, gate_moment, mine, sums):
    _, rows, block = arrived.shape
    rep = lax.axis_size("rep")
    r = lax.axis_index("rep")
    run = rec_moment.shape[0] // rep
    depth = rows - run
    half, share = block // 2, block // rep
    total = arrived[0]
    for i in range(1, arrived.shape[0]):
        total += arrived[i]
    rec_grad = total[:run]
    rec_pre = jnp.dot(
        rec_grad, rec_right[...].astype(F32), precision=HIGH, preferred_element_type=F32
    )
    start = pl.multiple_of(r * run, run)
    rec_new = BETA * rec_moment[pl.ds(start, run), :] + rec_pre
    mine[pl.ds(0, run), :] = rec_new

    gate_grad = total[run:, :half]
    packed = None
    for q in range(2):
        term = lax.dot_general(
            gate_moment[pl.ds(q * depth, depth), :],
            placing(block, share, q, r),
            ALONG_COLUMNS,
            precision=HIGH,
            preferred_element_type=F32,
        )
        packed = term if packed is None else packed + term
    gate_new = BETA * packed + total[run:, half:]
    mine[pl.ds(run, depth), pl.ds(0, half)] = gate_new
    mine[pl.ds(run, depth), pl.ds(half, half)] = gate_new

    row = lax.broadcasted_iota(jnp.int32, sums.shape[1:], 0)
    tile = jnp.zeros(sums.shape[1:], F32)
    for i, value in enumerate((rec_grad, rec_new, gate_grad, gate_new)):
        tile = jnp.where(row == i, square_sum(value), tile)
    for i in range(sums.shape[0]):
        sums[i] = tile


def update_kernel(
    sums,
    full,
    rec_weight,
    gate_weight,
    rec_new,
    rec_moment,
    rec_step,
    rec_copy,
    gate_new,
    gate_moment,
    gate_step,
    gate_copy,
):
    rep, rows, block = full.shape
    run = rec_weight.shape[0] // rep
    depth = rows - run
    half, share = block // 2, block // rep
    rec_value = full[:, pl.ds(0, run), :].reshape(rep * run, block)
    parts = []
    for q in range(2):
        part = None
        for r in range(rep):
            term = jnp.dot(
                full[r, pl.ds(run, depth), pl.ds(0, half)],
                placing(block, share, q, r),
                precision=HIGH,
                preferred_element_type=F32,
            )
            part = term if part is None else part + term
        parts.append(part)
    gate_value = jnp.concatenate(parts, axis=0)

    total = sums[0]
    for i in range(1, sums.shape[0]):
        total += sums[i]
    places = (
        (rec_value, rec_weight, rec_new, rec_moment, rec_step, rec_copy),
        (gate_value, gate_weight, gate_new, gate_moment, gate_step, gate_copy),
    )
    for i, (value, weight, new, moment, step, copy) in enumerate(places):
        scale = jnp.sqrt(total[2 * i : 2 * i + 1]) / jnp.sqrt(
            total[2 * i + 1 : 2 * i + 2] + EPSILON
        )
        scale = jnp.concatenate([LEARN_RATE * scale] * 2, axis=1)
        taken = scale * value
        result = weight[...] - taken
        moment[...] = value
        step[...] = taken
        new[...] = result
        copy[...] = result.astype(jnp.bfloat16)


def shards(
    normed,
    rec_cot,
    conv_out,
    gate_cot,
    rec_weight,
    rec_moment,
    rec_right,
    gate_weight,
    gate_moment,
    gate_left,
    gate_right,
):
    fs, rep = size_of(FS), lax.axis_size("rep")
    like = lambda value, kind=F32: jax.ShapeDtypeStruct(value.shape, kind)
    gate_weight, gate_moment = gate_weight[0], gate_moment[0]

    with jax.named_scope("product"):
        tiles = product(normed, rec_cot, conv_out, gate_cot, gate_right[0], rep)
    with jax.named_scope("near"):
        arrived = exchange(tiles, "rep")
    with jax.named_scope("left"):
        left = lax.all_gather(gate_left[0].astype(F32), FS, tiled=True).reshape(fs, *gate_left.shape[1:])
    with jax.named_scope("middle"):
        tiles = middle(arrived, left)
    with jax.named_scope("quarter"):
        hi, lo = lax.axis_size("fs_hi"), lax.axis_size("fs_lo")
        rows = tiles.shape[1]
        tiles = add_up(exchange(tiles.reshape(lo, hi * rows, -1), "fs_lo"))
    with jax.named_scope("far"):
        arrived = exchange(tiles.reshape(hi, rows, -1), "fs_hi")
    with jax.named_scope("settle"):
        mine, sums = on_core(
            settle_kernel,
            (
                jax.ShapeDtypeStruct(arrived.shape[1:], F32),
                jax.ShapeDtypeStruct((fs, 4, 128), F32),
            ),
            (arrived, rec_right, rec_moment, gate_moment),
        )
    with jax.named_scope("share"):
        full = lax.all_gather(mine, "rep")
    with jax.named_scope("sums"):
        sums = fold(exchange(sums, FS), rep * size_of(TP), full)
        sums = exchange(sums, ("rep", *TP))
    with jax.named_scope("update"):
        bf16 = jnp.bfloat16
        (
            rec_new,
            rec_moment_new,
            rec_step,
            rec_copy,
            gate_new,
            gate_moment_new,
            gate_step,
            gate_copy,
        ) = on_core(
            update_kernel,
            (
                like(rec_weight),
                like(rec_weight),
                like(rec_weight),
                like(rec_weight, bf16),
                like(gate_weight),
                like(gate_weight),
                like(gate_weight),
                like(gate_weight, bf16),
            ),
            (sums, full, rec_weight, gate_weight),
        )
    return (
        rec_new,
        rec_moment_new,
        rec_step,
        rec_copy,
        gate_new[None],
        gate_moment_new[None],
        gate_step[None],
        gate_copy[None],
    )


def solution(mesh):
    fs, rep, tp = (mesh.shape[name] for name in ("fs", "rep", "tp"))
    split = Mesh(
        mesh.devices.reshape(fs // 4, 4, rep, tp // 2, 2),
        (*FS, "rep", *TP),
    )
    tokens = (*FS, "rep")
    placed = (
        P(tokens, None),
        P(tokens, TP),
        P(tokens, TP),
        P(tokens, TP),
        P(FS, TP),
        P(FS, TP),
        P(TP, None),
        P(TP, FS, None),
        P(TP, FS, None),
        P(TP, FS, None),
        P(TP, None, None),
    )

    return jax.shard_map(
        shards,
        mesh=split,
        in_specs=placed,
        out_specs=(P(FS, TP),) * 4 + (P(TP, FS, None),) * 4,
        check_vma=False,
    )
```

```python
import jax
import jax.numpy as jnp
from jax import lax
from jax.experimental import pallas as pl
from jax.experimental.pallas import tpu as pltpu
from jax.sharding import Mesh
from jax.sharding import PartitionSpec as P

CORE = ("fs", "tp_1")
QUARTER = 4
TP = ("tp_0", "tp_1")

BETA = 0.9
LEARN_RATE = 0.02
EPSILON = 1e-06
PIECES = 4
GRANT = 16 << 20
F32 = jnp.float32
HIGH = lax.Precision.HIGHEST
ALONG_ROWS = (((0,), (0,)), ((), ()))
ALONG_COLUMNS = (((1,), (1,)), ((), ()))


def size_of(axes):
    axes = (axes,) if isinstance(axes, str) else axes
    size = 1
    for axis in axes:
        size *= lax.axis_size(axis)
    return size


def exchange(tiles, axes, groups=None):
    return lax.all_to_all(
        tiles,
        axes,
        split_axis=0,
        concat_axis=0,
        tiled=True,
        axis_index_groups=groups,
    )


def chip_at(hi, lo, core, fs):
    return (hi * QUARTER + lo + core * (QUARTER // 2)) % fs


def z_groups(fs, cores, within):
    hi, lo = fs // QUARTER, QUARTER
    place = lambda h, l, c: chip_at(h, l, c, fs) * cores + c
    if within:
        return [
            [place(h, l, c) for l in range(lo)] for h in range(hi) for c in range(cores)
        ]
    return [
        [place(h, l, c) for h in range(hi)] for l in range(lo) for c in range(cores)
    ]


def whole():
    return pl.BlockSpec(memory_space=pltpu.VMEM)


def on_core(kernel, outs, args, scratch=(), flops=1 << 26):
    moved = sum(a.size * a.dtype.itemsize for a in (*args, *outs))
    single = len(outs) == 1
    return pl.pallas_call(
        kernel,
        out_shape=outs[0] if single else outs,
        in_specs=[whole() for _ in args],
        out_specs=whole() if single else [whole() for _ in outs],
        scratch_shapes=list(scratch),
        compiler_params=pltpu.CompilerParams(vmem_limit_bytes=GRANT),
        cost_estimate=pl.CostEstimate(
            flops=flops, bytes_accessed=moved, transcendentals=0
        ),
    )(*args)


def product_kernel(
    normed_hbm,
    cot_hbm,
    conv_hbm,
    gate_hbm,
    right_hbm,
    tiles_hbm,
    normed,
    rec_cot,
    conv_out,
    gate_cot,
    right,
    tiles,
    in_sems,
    out_sems,
):
    rep, rows, block = tiles.shape
    share = block // rep
    rec_rows = rows - 2 * share
    step = rec_rows // PIECES
    run = 128 // rep

    small = [
        pltpu.make_async_copy(source, target, in_sems.at[i])
        for i, (source, target) in enumerate(
            (
                (conv_hbm, conv_out),
                (gate_hbm, gate_cot),
                (right_hbm, right),
                (cot_hbm, rec_cot),
            )
        )
    ]
    large = pltpu.make_async_copy(normed_hbm, normed, in_sems.at[len(small)])
    for copy in (*small, large):
        copy.start()

    def send(start, size, i):
        part = (slice(None), pl.ds(start, size), slice(None))
        copy = pltpu.make_async_copy(tiles.at[part], tiles_hbm.at[part], out_sems.at[i])
        copy.start()
        return copy

    sent = []
    for copy in small:
        copy.wait()
    grad = lax.dot_general(
        gate_cot[...], conv_out[...], ALONG_ROWS, preferred_element_type=F32
    )
    done = lax.dot_general(
        right[...].astype(F32),
        grad,
        ALONG_ROWS,
        precision=HIGH,
        preferred_element_type=F32,
    )
    for r in range(rep):
        for i, value in enumerate((grad, done)):
            tiles[r, pl.ds(rec_rows + i * share, share), :] = value[
                r * share : (r + 1) * share
            ]
    sent.append(send(rec_rows, 2 * share, PIECES))
    large.wait()
    part = lax.dot_general(
        normed[...], rec_cot[...], ALONG_ROWS, preferred_element_type=F32
    )
    for piece in range(PIECES):
        for owner in range(piece * step // run, (piece + 1) * step // run):
            for r in range(rep):
                start = (owner * rep + r) * run
                tiles[r, pl.ds(owner * run, run), :] = part[start : start + run]
        sent.append(send(piece * step, step, piece))
    for copy in sent:
        copy.wait()


def product(normed, rec_cot, conv_out, gate_cot, right, rep):
    tokens, width = normed.shape
    block = rec_cot.shape[1]
    rows = (width + 2 * block) // rep
    args = (normed, rec_cot, conv_out, gate_cot, right)
    return pl.pallas_call(
        product_kernel,
        in_specs=[pl.BlockSpec(memory_space=pl.ANY)] * len(args),
        out_specs=pl.BlockSpec(memory_space=pl.ANY),
        out_shape=jax.ShapeDtypeStruct((rep, rows, block), F32),
        scratch_shapes=[
            *[pltpu.VMEM(value.shape, value.dtype) for value in args],
            pltpu.VMEM((rep, rows, block), F32),
            pltpu.SemaphoreType.DMA((len(args),)),
            pltpu.SemaphoreType.DMA((PIECES + 1,)),
        ],
        cost_estimate=pl.CostEstimate(
            flops=2 * tokens * block * (width + block),
            bytes_accessed=1 << 22,
            transcendentals=0,
        ),
    )(*args)


def middle_kernel(arrived, left, tiles):
    rep = arrived.shape[0]
    fs, _, block = tiles.shape
    half, share = block // 2, block // rep
    rec_rows = arrived.shape[1] - 2 * share
    run = rec_rows // fs

    def total(start, size):
        value = arrived[0, pl.ds(start, size), :]
        for r in range(1, rep):
            value += arrived[r, pl.ds(start, size), :]
        return value

    core = lax.axis_index("tp_1")
    hi = fs // QUARTER
    place = []
    for f in range(fs):
        at = lax.rem(f + fs - core * (QUARTER // 2), fs)
        place.append(lax.rem(at, QUARTER) * hi + lax.div(at, QUARTER))
    for f in range(fs):
        tiles[place[f], pl.ds(0, run), :] = total(f * run, run)
    turned = total(rec_rows, share)
    right_done = total(rec_rows + share, share)
    blank = jnp.zeros_like(right_done)
    depth = left.shape[1] // 2
    done = None
    for q in range(2):
        rows_q = left[:, pl.ds(q * depth, depth), :].reshape(fs * depth, block)
        wide = [blank] * q + [right_done] + [blank] * (1 - q)
        term = lax.dot_general(
            rows_q,
            jnp.concatenate(wide, axis=0),
            ALONG_COLUMNS,
            precision=HIGH,
            preferred_element_type=F32,
        )
        done = term if done is None else done + term
    for f in range(fs):
        row, side = f // 2 * depth, f % 2 * half
        tiles[place[f], pl.ds(run, depth), pl.ds(0, half)] = turned[
            row : row + depth, side : side + half
        ]
        tiles[place[f], pl.ds(run, depth), pl.ds(half, half)] = done[
            f * depth : (f + 1) * depth
        ]


def middle(arrived, left):
    fs, own_rows, block = left.shape
    rec_rows = arrived.shape[1] - 2 * block // arrived.shape[0]
    out = jax.ShapeDtypeStruct((fs, rec_rows // fs + own_rows // 2, block), F32)
    return on_core(middle_kernel, (out,), (arrived, left), flops=1 << 30)


def add_kernel(tiles, total):
    value = tiles[0]
    for i in range(1, tiles.shape[0]):
        value += tiles[i]
    total[...] = value


def add_up(tiles):
    return on_core(
        add_kernel, (jax.ShapeDtypeStruct(tiles.shape[1:], F32),), (tiles,)
    )


def fold_kernel(tiles, after, copies):
    total = tiles[0]
    for i in range(1, tiles.shape[0]):
        total += tiles[i]
    for i in range(copies.shape[0]):
        copies[i] = total


def fold(tiles, count, after):
    out = jax.ShapeDtypeStruct((count, *tiles.shape[1:]), F32)
    return on_core(fold_kernel, (out,), (tiles, after))


def square_sum(value):
    return jnp.sum(jnp.sum(value * value, axis=0, keepdims=True), axis=1, keepdims=True)


def placing(block, share, q, r):
    lane = lax.broadcasted_iota(jnp.int32, (2 * share, block), 0) - q * share
    column = lax.broadcasted_iota(jnp.int32, (2 * share, block), 1) - r * share
    inside = (lane >= 0) & (lane < share)
    return jnp.where(inside & (lane == column), 1.0, 0.0).astype(F32)


def settle_kernel(arrived, rec_right, rec_moment, gate_moment, mine, sums):
    _, rows, block = arrived.shape
    rep = lax.axis_size("rep")
    r = lax.axis_index("rep")
    run = rec_moment.shape[0] // rep
    depth = rows - run
    half, share = block // 2, block // rep
    total = arrived[0]
    for i in range(1, arrived.shape[0]):
        total += arrived[i]
    rec_grad = total[:run]
    rec_pre = jnp.dot(
        rec_grad, rec_right[...].astype(F32), precision=HIGH, preferred_element_type=F32
    )
    start = pl.multiple_of(r * run, run)
    rec_new = BETA * rec_moment[pl.ds(start, run), :] + rec_pre
    mine[pl.ds(0, run), :] = rec_new

    gate_grad = total[run:, :half]
    packed = None
    for q in range(2):
        term = lax.dot_general(
            gate_moment[pl.ds(q * depth, depth), :],
            placing(block, share, q, r),
            ALONG_COLUMNS,
            precision=HIGH,
            preferred_element_type=F32,
        )
        packed = term if packed is None else packed + term
    gate_new = BETA * packed + total[run:, half:]
    mine[pl.ds(run, depth), pl.ds(0, half)] = gate_new
    mine[pl.ds(run, depth), pl.ds(half, half)] = gate_new

    row = lax.broadcasted_iota(jnp.int32, sums.shape[1:], 0)
    tile = jnp.zeros(sums.shape[1:], F32)
    for i, value in enumerate((rec_grad, rec_new, gate_grad, gate_new)):
        tile = jnp.where(row == i, square_sum(value), tile)
    for i in range(sums.shape[0]):
        sums[i] = tile


def update_kernel(
    sums,
    full,
    rec_weight,
    gate_weight,
    rec_new,
    rec_moment,
    rec_step,
    rec_copy,
    gate_new,
    gate_moment,
    gate_step,
    gate_copy,
):
    rep, rows, block = full.shape
    run = rec_weight.shape[0] // rep
    depth = rows - run
    half, share = block // 2, block // rep
    rec_value = full[:, pl.ds(0, run), :].reshape(rep * run, block)
    parts = []
    for q in range(2):
        part = None
        for r in range(rep):
            term = jnp.dot(
                full[r, pl.ds(run, depth), pl.ds(0, half)],
                placing(block, share, q, r),
                precision=HIGH,
                preferred_element_type=F32,
            )
            part = term if part is None else part + term
        parts.append(part)
    gate_value = jnp.concatenate(parts, axis=0)

    total = sums[0]
    for i in range(1, sums.shape[0]):
        total += sums[i]
    places = (
        (rec_value, rec_weight, rec_new, rec_moment, rec_step, rec_copy),
        (gate_value, gate_weight, gate_new, gate_moment, gate_step, gate_copy),
    )
    for i, (value, weight, new, moment, step, copy) in enumerate(places):
        scale = jnp.sqrt(total[2 * i : 2 * i + 1]) / jnp.sqrt(
            total[2 * i + 1 : 2 * i + 2] + EPSILON
        )
        scale = jnp.concatenate([LEARN_RATE * scale] * 2, axis=1)
        taken = scale * value
        result = weight[...] - taken
        moment[...] = value
        step[...] = taken
        new[...] = result
        copy[...] = result.astype(jnp.bfloat16)


def shards(
    normed,
    rec_cot,
    conv_out,
    gate_cot,
    rec_weight,
    rec_moment,
    rec_right,
    gate_weight,
    gate_moment,
    gate_left,
    gate_right,
):
    fs, rep = lax.axis_size("fs"), lax.axis_size("rep")
    like = lambda value, kind=F32: jax.ShapeDtypeStruct(value.shape, kind)
    gate_weight, gate_moment = gate_weight[0], gate_moment[0]

    with jax.named_scope("product"):
        tiles = product(normed, rec_cot, conv_out, gate_cot, gate_right[0], rep)
    with jax.named_scope("near"):
        arrived = exchange(tiles, "rep")
    with jax.named_scope("left"):
        left = lax.all_gather(gate_left[0].astype(F32), "fs", tiled=True).reshape(fs, *gate_left.shape[1:])
    with jax.named_scope("middle"):
        tiles = middle(arrived, left)
    with jax.named_scope("quarter"):
        hi, lo, cores = fs // QUARTER, QUARTER, lax.axis_size("tp_1")
        rows = tiles.shape[1]
        tiles = tiles.reshape(lo, hi * rows, -1)
        tiles = add_up(exchange(tiles, CORE, z_groups(fs, cores, True)))
    with jax.named_scope("far"):
        tiles = tiles.reshape(hi, rows, -1)
        arrived = exchange(tiles, CORE, z_groups(fs, cores, False))
    with jax.named_scope("settle"):
        mine, sums = on_core(
            settle_kernel,
            (
                jax.ShapeDtypeStruct(arrived.shape[1:], F32),
                jax.ShapeDtypeStruct((fs, 4, 128), F32),
            ),
            (arrived, rec_right, rec_moment, gate_moment),
        )
    with jax.named_scope("share"):
        full = lax.all_gather(mine, "rep")
    with jax.named_scope("sums"):
        sums = fold(exchange(sums, "fs"), rep * size_of(TP), full)
        sums = exchange(sums, ("rep", *TP))
    with jax.named_scope("update"):
        bf16 = jnp.bfloat16
        (
            rec_new,
            rec_moment_new,
            rec_step,
            rec_copy,
            gate_new,
            gate_moment_new,
            gate_step,
            gate_copy,
        ) = on_core(
            update_kernel,
            (
                like(rec_weight),
                like(rec_weight),
                like(rec_weight),
                like(rec_weight, bf16),
                like(gate_weight),
                like(gate_weight),
                like(gate_weight),
                like(gate_weight, bf16),
            ),
            (sums, full, rec_weight, gate_weight),
        )
    return (
        rec_new,
        rec_moment_new,
        rec_step,
        rec_copy,
        gate_new[None],
        gate_moment_new[None],
        gate_step[None],
        gate_copy[None],
    )


def solution(mesh):
    fs, rep, tp = (mesh.shape[name] for name in ("fs", "rep", "tp"))
    split = Mesh(
        mesh.devices.reshape(fs, rep, tp // 2, 2),
        ("fs", "rep", *TP),
    )
    tokens = ("fs", "rep")
    placed = (
        P(tokens, None),
        P(tokens, TP),
        P(tokens, TP),
        P(tokens, TP),
        P("fs", TP),
        P("fs", TP),
        P(TP, None),
        P(TP, "fs", None),
        P(TP, "fs", None),
        P(TP, "fs", None),
        P(TP, None, None),
    )

    return jax.shard_map(
        shards,
        mesh=split,
        in_specs=placed,
        out_specs=(P("fs", TP),) * 4 + (P(TP, "fs", None),) * 4,
        check_vma=False,
    )
```

```python
import jax
import jax.numpy as jnp
from jax import lax
from jax.experimental import pallas as pl
from jax.experimental.pallas import tpu as pltpu
from jax.sharding import Mesh
from jax.sharding import PartitionSpec as P

CORE = ("fs", "tp_1")
SPAN = 2
TP = ("tp_0", "tp_1")

BETA = 0.9
LEARN_RATE = 0.02
EPSILON = 1e-06
PIECES = 4
GRANT = 16 << 20
F32 = jnp.float32
HIGH = lax.Precision.HIGHEST
ALONG_ROWS = (((0,), (0,)), ((), ()))
ALONG_COLUMNS = (((1,), (1,)), ((), ()))


def size_of(axes):
    axes = (axes,) if isinstance(axes, str) else axes
    size = 1
    for axis in axes:
        size *= lax.axis_size(axis)
    return size


def exchange(tiles, axes, groups=None):
    return lax.all_to_all(
        tiles,
        axes,
        split_axis=0,
        concat_axis=0,
        tiled=True,
        axis_index_groups=groups,
    )


def chip_at(hi, lo, core, fs):
    return (hi * SPAN + lo + core * (SPAN // 2)) % fs


def z_groups(fs, cores, within):
    hi, lo = fs // SPAN, SPAN
    place = lambda h, l, c: chip_at(h, l, c, fs) * cores + c
    if within:
        return [
            [place(h, l, c) for l in range(lo)] for h in range(hi) for c in range(cores)
        ]
    return [
        [place(h, l, c) for h in range(hi)] for l in range(lo) for c in range(cores)
    ]


def whole():
    return pl.BlockSpec(memory_space=pltpu.VMEM)


def on_core(kernel, outs, args, scratch=(), flops=1 << 26):
    moved = sum(a.size * a.dtype.itemsize for a in (*args, *outs))
    single = len(outs) == 1
    return pl.pallas_call(
        kernel,
        out_shape=outs[0] if single else outs,
        in_specs=[whole() for _ in args],
        out_specs=whole() if single else [whole() for _ in outs],
        scratch_shapes=list(scratch),
        compiler_params=pltpu.CompilerParams(vmem_limit_bytes=GRANT),
        cost_estimate=pl.CostEstimate(
            flops=flops, bytes_accessed=moved, transcendentals=0
        ),
    )(*args)


def product_kernel(
    normed_hbm,
    cot_hbm,
    conv_hbm,
    gate_hbm,
    right_hbm,
    tiles_hbm,
    normed,
    rec_cot,
    conv_out,
    gate_cot,
    right,
    tiles,
    in_sems,
    out_sems,
):
    rep, rows, block = tiles.shape
    share = block // rep
    rec_rows = rows - 2 * share
    step = rec_rows // PIECES
    run = 128 // rep

    small = [
        pltpu.make_async_copy(source, target, in_sems.at[i])
        for i, (source, target) in enumerate(
            (
                (conv_hbm, conv_out),
                (gate_hbm, gate_cot),
                (right_hbm, right),
                (cot_hbm, rec_cot),
            )
        )
    ]
    large = pltpu.make_async_copy(normed_hbm, normed, in_sems.at[len(small)])
    for copy in (*small, large):
        copy.start()

    def send(start, size, i):
        part = (slice(None), pl.ds(start, size), slice(None))
        copy = pltpu.make_async_copy(tiles.at[part], tiles_hbm.at[part], out_sems.at[i])
        copy.start()
        return copy

    sent = []
    for copy in small:
        copy.wait()
    grad = lax.dot_general(
        gate_cot[...], conv_out[...], ALONG_ROWS, preferred_element_type=F32
    )
    done = lax.dot_general(
        right[...].astype(F32),
        grad,
        ALONG_ROWS,
        precision=HIGH,
        preferred_element_type=F32,
    )
    for r in range(rep):
        for i, value in enumerate((grad, done)):
            tiles[r, pl.ds(rec_rows + i * share, share), :] = value[
                r * share : (r + 1) * share
            ]
    sent.append(send(rec_rows, 2 * share, PIECES))
    large.wait()
    part = lax.dot_general(
        normed[...], rec_cot[...], ALONG_ROWS, preferred_element_type=F32
    )
    for piece in range(PIECES):
        for owner in range(piece * step // run, (piece + 1) * step // run):
            for r in range(rep):
                start = (owner * rep + r) * run
                tiles[r, pl.ds(owner * run, run), :] = part[start : start + run]
        sent.append(send(piece * step, step, piece))
    for copy in sent:
        copy.wait()


def product(normed, rec_cot, conv_out, gate_cot, right, rep):
    tokens, width = normed.shape
    block = rec_cot.shape[1]
    rows = (width + 2 * block) // rep
    args = (normed, rec_cot, conv_out, gate_cot, right)
    return pl.pallas_call(
        product_kernel,
        in_specs=[pl.BlockSpec(memory_space=pl.ANY)] * len(args),
        out_specs=pl.BlockSpec(memory_space=pl.ANY),
        out_shape=jax.ShapeDtypeStruct((rep, rows, block), F32),
        scratch_shapes=[
            *[pltpu.VMEM(value.shape, value.dtype) for value in args],
            pltpu.VMEM((rep, rows, block), F32),
            pltpu.SemaphoreType.DMA((len(args),)),
            pltpu.SemaphoreType.DMA((PIECES + 1,)),
        ],
        cost_estimate=pl.CostEstimate(
            flops=2 * tokens * block * (width + block),
            bytes_accessed=1 << 22,
            transcendentals=0,
        ),
    )(*args)


def middle_kernel(arrived, left, tiles):
    rep = arrived.shape[0]
    fs, _, block = tiles.shape
    half, share = block // 2, block // rep
    rec_rows = arrived.shape[1] - 2 * share
    run = rec_rows // fs

    def total(start, size):
        value = arrived[0, pl.ds(start, size), :]
        for r in range(1, rep):
            value += arrived[r, pl.ds(start, size), :]
        return value

    core = lax.axis_index("tp_1")
    hi = fs // SPAN
    place = []
    for f in range(fs):
        at = lax.rem(f + fs - core * (SPAN // 2), fs)
        place.append(lax.rem(at, SPAN) * hi + lax.div(at, SPAN))
    for f in range(fs):
        tiles[place[f], pl.ds(0, run), :] = total(f * run, run)
    turned = total(rec_rows, share)
    right_done = total(rec_rows + share, share)
    blank = jnp.zeros_like(right_done)
    depth = left.shape[1] // 2
    done = None
    for q in range(2):
        rows_q = left[:, pl.ds(q * depth, depth), :].reshape(fs * depth, block)
        wide = [blank] * q + [right_done] + [blank] * (1 - q)
        term = lax.dot_general(
            rows_q,
            jnp.concatenate(wide, axis=0),
            ALONG_COLUMNS,
            precision=HIGH,
            preferred_element_type=F32,
        )
        done = term if done is None else done + term
    for f in range(fs):
        row, side = f // 2 * depth, f % 2 * half
        tiles[place[f], pl.ds(run, depth), pl.ds(0, half)] = turned[
            row : row + depth, side : side + half
        ]
        tiles[place[f], pl.ds(run, depth), pl.ds(half, half)] = done[
            f * depth : (f + 1) * depth
        ]


def middle(arrived, left):
    fs, own_rows, block = left.shape
    rec_rows = arrived.shape[1] - 2 * block // arrived.shape[0]
    out = jax.ShapeDtypeStruct((fs, rec_rows // fs + own_rows // 2, block), F32)
    return on_core(middle_kernel, (out,), (arrived, left), flops=1 << 30)


def add_kernel(tiles, total):
    value = tiles[0]
    for i in range(1, tiles.shape[0]):
        value += tiles[i]
    total[...] = value


def add_up(tiles):
    return on_core(
        add_kernel, (jax.ShapeDtypeStruct(tiles.shape[1:], F32),), (tiles,)
    )


def fold_kernel(tiles, after, copies):
    total = tiles[0]
    for i in range(1, tiles.shape[0]):
        total += tiles[i]
    for i in range(copies.shape[0]):
        copies[i] = total


def fold(tiles, count, after):
    out = jax.ShapeDtypeStruct((count, *tiles.shape[1:]), F32)
    return on_core(fold_kernel, (out,), (tiles, after))


def square_sum(value):
    return jnp.sum(jnp.sum(value * value, axis=0, keepdims=True), axis=1, keepdims=True)


def placing(block, share, q, r):
    lane = lax.broadcasted_iota(jnp.int32, (2 * share, block), 0) - q * share
    column = lax.broadcasted_iota(jnp.int32, (2 * share, block), 1) - r * share
    inside = (lane >= 0) & (lane < share)
    return jnp.where(inside & (lane == column), 1.0, 0.0).astype(F32)


def settle_kernel(arrived, rec_right, rec_moment, gate_moment, mine, sums):
    _, rows, block = arrived.shape
    rep = lax.axis_size("rep")
    r = lax.axis_index("rep")
    run = rec_moment.shape[0] // rep
    depth = rows - run
    half, share = block // 2, block // rep
    total = arrived[0]
    for i in range(1, arrived.shape[0]):
        total += arrived[i]
    rec_grad = total[:run]
    rec_pre = jnp.dot(
        rec_grad, rec_right[...].astype(F32), precision=HIGH, preferred_element_type=F32
    )
    start = pl.multiple_of(r * run, run)
    rec_new = BETA * rec_moment[pl.ds(start, run), :] + rec_pre
    mine[pl.ds(0, run), :] = rec_new

    gate_grad = total[run:, :half]
    packed = None
    for q in range(2):
        term = lax.dot_general(
            gate_moment[pl.ds(q * depth, depth), :],
            placing(block, share, q, r),
            ALONG_COLUMNS,
            precision=HIGH,
            preferred_element_type=F32,
        )
        packed = term if packed is None else packed + term
    gate_new = BETA * packed + total[run:, half:]
    mine[pl.ds(run, depth), pl.ds(0, half)] = gate_new
    mine[pl.ds(run, depth), pl.ds(half, half)] = gate_new

    row = lax.broadcasted_iota(jnp.int32, sums.shape[1:], 0)
    tile = jnp.zeros(sums.shape[1:], F32)
    for i, value in enumerate((rec_grad, rec_new, gate_grad, gate_new)):
        tile = jnp.where(row == i, square_sum(value), tile)
    for i in range(sums.shape[0]):
        sums[i] = tile


def update_kernel(
    sums,
    full,
    rec_weight,
    gate_weight,
    rec_new,
    rec_moment,
    rec_step,
    rec_copy,
    gate_new,
    gate_moment,
    gate_step,
    gate_copy,
):
    rep, rows, block = full.shape
    run = rec_weight.shape[0] // rep
    depth = rows - run
    half, share = block // 2, block // rep
    rec_value = full[:, pl.ds(0, run), :].reshape(rep * run, block)
    parts = []
    for q in range(2):
        part = None
        for r in range(rep):
            term = jnp.dot(
                full[r, pl.ds(run, depth), pl.ds(0, half)],
                placing(block, share, q, r),
                precision=HIGH,
                preferred_element_type=F32,
            )
            part = term if part is None else part + term
        parts.append(part)
    gate_value = jnp.concatenate(parts, axis=0)

    total = sums[0]
    for i in range(1, sums.shape[0]):
        total += sums[i]
    places = (
        (rec_value, rec_weight, rec_new, rec_moment, rec_step, rec_copy),
        (gate_value, gate_weight, gate_new, gate_moment, gate_step, gate_copy),
    )
    for i, (value, weight, new, moment, step, copy) in enumerate(places):
        scale = jnp.sqrt(total[2 * i : 2 * i + 1]) / jnp.sqrt(
            total[2 * i + 1 : 2 * i + 2] + EPSILON
        )
        scale = jnp.concatenate([LEARN_RATE * scale] * 2, axis=1)
        taken = scale * value
        result = weight[...] - taken
        moment[...] = value
        step[...] = taken
        new[...] = result
        copy[...] = result.astype(jnp.bfloat16)


def shards(
    normed,
    rec_cot,
    conv_out,
    gate_cot,
    rec_weight,
    rec_moment,
    rec_right,
    gate_weight,
    gate_moment,
    gate_left,
    gate_right,
):
    fs, rep = lax.axis_size("fs"), lax.axis_size("rep")
    like = lambda value, kind=F32: jax.ShapeDtypeStruct(value.shape, kind)
    gate_weight, gate_moment = gate_weight[0], gate_moment[0]

    with jax.named_scope("product"):
        tiles = product(normed, rec_cot, conv_out, gate_cot, gate_right[0], rep)
    with jax.named_scope("near"):
        arrived = exchange(tiles, "rep")
    with jax.named_scope("left"):
        left = lax.all_gather(gate_left[0].astype(F32), "fs", tiled=True).reshape(fs, *gate_left.shape[1:])
    with jax.named_scope("middle"):
        tiles = middle(arrived, left)
    with jax.named_scope("quarter"):
        hi, lo, cores = fs // SPAN, SPAN, lax.axis_size("tp_1")
        rows = tiles.shape[1]
        tiles = tiles.reshape(lo, hi * rows, -1)
        tiles = add_up(exchange(tiles, CORE, z_groups(fs, cores, True)))
    with jax.named_scope("far"):
        tiles = tiles.reshape(hi, rows, -1)
        arrived = exchange(tiles, CORE, z_groups(fs, cores, False))
    with jax.named_scope("settle"):
        mine, sums = on_core(
            settle_kernel,
            (
                jax.ShapeDtypeStruct(arrived.shape[1:], F32),
                jax.ShapeDtypeStruct((fs, 4, 128), F32),
            ),
            (arrived, rec_right, rec_moment, gate_moment),
        )
    with jax.named_scope("share"):
        full = lax.all_gather(mine, "rep")
    with jax.named_scope("sums"):
        sums = fold(exchange(sums, "fs"), rep * size_of(TP), full)
        sums = exchange(sums, ("rep", *TP))
    with jax.named_scope("update"):
        bf16 = jnp.bfloat16
        (
            rec_new,
            rec_moment_new,
            rec_step,
            rec_copy,
            gate_new,
            gate_moment_new,
            gate_step,
            gate_copy,
        ) = on_core(
            update_kernel,
            (
                like(rec_weight),
                like(rec_weight),
                like(rec_weight),
                like(rec_weight, bf16),
                like(gate_weight),
                like(gate_weight),
                like(gate_weight),
                like(gate_weight, bf16),
            ),
            (sums, full, rec_weight, gate_weight),
        )
    return (
        rec_new,
        rec_moment_new,
        rec_step,
        rec_copy,
        gate_new[None],
        gate_moment_new[None],
        gate_step[None],
        gate_copy[None],
    )


def solution(mesh):
    fs, rep, tp = (mesh.shape[name] for name in ("fs", "rep", "tp"))
    split = Mesh(
        mesh.devices.reshape(fs, rep, tp // 2, 2),
        ("fs", "rep", *TP),
    )
    tokens = ("fs", "rep")
    placed = (
        P(tokens, None),
        P(tokens, TP),
        P(tokens, TP),
        P(tokens, TP),
        P("fs", TP),
        P("fs", TP),
        P(TP, None),
        P(TP, "fs", None),
        P(TP, "fs", None),
        P(TP, "fs", None),
        P(TP, None, None),
    )

    return jax.shard_map(
        shards,
        mesh=split,
        in_specs=placed,
        out_specs=(P("fs", TP),) * 4 + (P(TP, "fs", None),) * 4,
        check_vma=False,
    )
```

```python
import jax
import jax.numpy as jnp
from jax import lax
from jax.experimental import pallas as pl
from jax.experimental.pallas import tpu as pltpu
from jax.sharding import Mesh
from jax.sharding import PartitionSpec as P

CORE = ("fs", "tp_1")
PLANE = ("rep", "tp_0")
SPAN = 2
TP = ("tp_0", "tp_1")

BETA = 0.9
LEARN_RATE = 0.02
EPSILON = 1e-06
PIECES = 4
GRANT = 16 << 20
F32 = jnp.float32
HIGH = lax.Precision.HIGHEST
ALONG_ROWS = (((0,), (0,)), ((), ()))
ALONG_COLUMNS = (((1,), (1,)), ((), ()))


def size_of(axes):
    axes = (axes,) if isinstance(axes, str) else axes
    size = 1
    for axis in axes:
        size *= lax.axis_size(axis)
    return size


def exchange(tiles, axes, groups=None):
    return lax.all_to_all(
        tiles,
        axes,
        split_axis=0,
        concat_axis=0,
        tiled=True,
        axis_index_groups=groups,
    )


def chip_at(hi, lo, core, fs):
    return (hi * SPAN + lo + core * (SPAN // 2)) % fs


def z_groups(fs, cores, within):
    hi, lo = fs // SPAN, SPAN
    place = lambda h, l, c: chip_at(h, l, c, fs) * cores + c
    if within:
        return [
            [place(h, l, c) for l in range(lo)] for h in range(hi) for c in range(cores)
        ]
    return [
        [place(h, l, c) for h in range(hi)] for l in range(lo) for c in range(cores)
    ]


def whole():
    return pl.BlockSpec(memory_space=pltpu.VMEM)


def on_core(kernel, outs, args, scratch=(), flops=1 << 26):
    moved = sum(a.size * a.dtype.itemsize for a in (*args, *outs))
    single = len(outs) == 1
    return pl.pallas_call(
        kernel,
        out_shape=outs[0] if single else outs,
        in_specs=[whole() for _ in args],
        out_specs=whole() if single else [whole() for _ in outs],
        scratch_shapes=list(scratch),
        compiler_params=pltpu.CompilerParams(vmem_limit_bytes=GRANT),
        cost_estimate=pl.CostEstimate(
            flops=flops, bytes_accessed=moved, transcendentals=0
        ),
    )(*args)


def product_kernel(
    normed_hbm,
    cot_hbm,
    conv_hbm,
    gate_hbm,
    right_hbm,
    tiles_hbm,
    normed,
    rec_cot,
    conv_out,
    gate_cot,
    right,
    tiles,
    in_sems,
    out_sems,
):
    rep, rows, block = tiles.shape
    share = block // rep
    rec_rows = rows - 2 * share
    step = rec_rows // PIECES
    run = 128 // rep

    small = [
        pltpu.make_async_copy(source, target, in_sems.at[i])
        for i, (source, target) in enumerate(
            (
                (conv_hbm, conv_out),
                (gate_hbm, gate_cot),
                (right_hbm, right),
                (cot_hbm, rec_cot),
            )
        )
    ]
    large = pltpu.make_async_copy(normed_hbm, normed, in_sems.at[len(small)])
    for copy in (*small, large):
        copy.start()

    def send(start, size, i):
        part = (slice(None), pl.ds(start, size), slice(None))
        copy = pltpu.make_async_copy(tiles.at[part], tiles_hbm.at[part], out_sems.at[i])
        copy.start()
        return copy

    sent = []
    for copy in small:
        copy.wait()
    grad = lax.dot_general(
        gate_cot[...], conv_out[...], ALONG_ROWS, preferred_element_type=F32
    )
    done = lax.dot_general(
        right[...].astype(F32),
        grad,
        ALONG_ROWS,
        precision=HIGH,
        preferred_element_type=F32,
    )
    for r in range(rep):
        for i, value in enumerate((grad, done)):
            tiles[r, pl.ds(rec_rows + i * share, share), :] = value[
                r * share : (r + 1) * share
            ]
    sent.append(send(rec_rows, 2 * share, PIECES))
    large.wait()
    part = lax.dot_general(
        normed[...], rec_cot[...], ALONG_ROWS, preferred_element_type=F32
    )
    for piece in range(PIECES):
        for owner in range(piece * step // run, (piece + 1) * step // run):
            for r in range(rep):
                start = (owner * rep + r) * run
                tiles[r, pl.ds(owner * run, run), :] = part[start : start + run]
        sent.append(send(piece * step, step, piece))
    for copy in sent:
        copy.wait()


def product(normed, rec_cot, conv_out, gate_cot, right, rep):
    tokens, width = normed.shape
    block = rec_cot.shape[1]
    rows = (width + 2 * block) // rep
    args = (normed, rec_cot, conv_out, gate_cot, right)
    return pl.pallas_call(
        product_kernel,
        in_specs=[pl.BlockSpec(memory_space=pl.ANY)] * len(args),
        out_specs=pl.BlockSpec(memory_space=pl.ANY),
        out_shape=jax.ShapeDtypeStruct((rep, rows, block), F32),
        scratch_shapes=[
            *[pltpu.VMEM(value.shape, value.dtype) for value in args],
            pltpu.VMEM((rep, rows, block), F32),
            pltpu.SemaphoreType.DMA((len(args),)),
            pltpu.SemaphoreType.DMA((PIECES + 1,)),
        ],
        cost_estimate=pl.CostEstimate(
            flops=2 * tokens * block * (width + block),
            bytes_accessed=1 << 22,
            transcendentals=0,
        ),
    )(*args)


def middle_kernel(arrived, left, tiles):
    rep = arrived.shape[0]
    fs, _, block = tiles.shape
    half, share = block // 2, block // rep
    rec_rows = arrived.shape[1] - 2 * share
    run = rec_rows // fs

    def total(start, size):
        value = arrived[0, pl.ds(start, size), :]
        for r in range(1, rep):
            value += arrived[r, pl.ds(start, size), :]
        return value

    core = lax.axis_index("tp_1")
    hi = fs // SPAN
    place = []
    for f in range(fs):
        at = lax.rem(f + fs - core * (SPAN // 2), fs)
        place.append(lax.rem(at, SPAN) * hi + lax.div(at, SPAN))
    for f in range(fs):
        tiles[place[f], pl.ds(0, run), :] = total(f * run, run)
    turned = total(rec_rows, share)
    right_done = total(rec_rows + share, share)
    blank = jnp.zeros_like(right_done)
    depth = left.shape[1] // 2
    done = None
    for q in range(2):
        rows_q = left[:, pl.ds(q * depth, depth), :].reshape(fs * depth, block)
        wide = [blank] * q + [right_done] + [blank] * (1 - q)
        term = lax.dot_general(
            rows_q,
            jnp.concatenate(wide, axis=0),
            ALONG_COLUMNS,
            precision=HIGH,
            preferred_element_type=F32,
        )
        done = term if done is None else done + term
    for f in range(fs):
        row, side = f // 2 * depth, f % 2 * half
        tiles[place[f], pl.ds(run, depth), pl.ds(0, half)] = turned[
            row : row + depth, side : side + half
        ]
        tiles[place[f], pl.ds(run, depth), pl.ds(half, half)] = done[
            f * depth : (f + 1) * depth
        ]


def middle(arrived, left):
    fs, own_rows, block = left.shape
    rec_rows = arrived.shape[1] - 2 * block // arrived.shape[0]
    out = jax.ShapeDtypeStruct((fs, rec_rows // fs + own_rows // 2, block), F32)
    return on_core(middle_kernel, (out,), (arrived, left), flops=1 << 30)


def add_kernel(tiles, total):
    value = tiles[0]
    for i in range(1, tiles.shape[0]):
        value += tiles[i]
    total[...] = value


def add_up(tiles):
    return on_core(
        add_kernel, (jax.ShapeDtypeStruct(tiles.shape[1:], F32),), (tiles,)
    )


def fold_kernel(tiles, after, copies):
    total = tiles[0]
    for i in range(1, tiles.shape[0]):
        total += tiles[i]
    for i in range(copies.shape[0]):
        copies[i] = total


def fold(tiles, count, after):
    out = jax.ShapeDtypeStruct((count, *tiles.shape[1:]), F32)
    return on_core(fold_kernel, (out,), (tiles, after))


def square_sum(value):
    return jnp.sum(jnp.sum(value * value, axis=0, keepdims=True), axis=1, keepdims=True)


def placing(block, share, q, r):
    lane = lax.broadcasted_iota(jnp.int32, (2 * share, block), 0) - q * share
    column = lax.broadcasted_iota(jnp.int32, (2 * share, block), 1) - r * share
    inside = (lane >= 0) & (lane < share)
    return jnp.where(inside & (lane == column), 1.0, 0.0).astype(F32)


def settle_kernel(arrived, rec_right, rec_moment, gate_moment, mine, sums):
    _, rows, block = arrived.shape
    rep = lax.axis_size("rep")
    r = lax.axis_index("rep")
    run = rec_moment.shape[0] // rep
    depth = rows - run
    half, share = block // 2, block // rep
    total = arrived[0]
    for i in range(1, arrived.shape[0]):
        total += arrived[i]
    rec_grad = total[:run]
    rec_pre = jnp.dot(
        rec_grad, rec_right[...].astype(F32), precision=HIGH, preferred_element_type=F32
    )
    start = pl.multiple_of(r * run, run)
    rec_new = BETA * rec_moment[pl.ds(start, run), :] + rec_pre
    mine[pl.ds(0, run), :] = rec_new

    gate_grad = total[run:, :half]
    packed = None
    for q in range(2):
        term = lax.dot_general(
            gate_moment[pl.ds(q * depth, depth), :],
            placing(block, share, q, r),
            ALONG_COLUMNS,
            precision=HIGH,
            preferred_element_type=F32,
        )
        packed = term if packed is None else packed + term
    gate_new = BETA * packed + total[run:, half:]
    mine[pl.ds(run, depth), pl.ds(0, half)] = gate_new
    mine[pl.ds(run, depth), pl.ds(half, half)] = gate_new

    row = lax.broadcasted_iota(jnp.int32, sums.shape[1:], 0)
    tile = jnp.zeros(sums.shape[1:], F32)
    for i, value in enumerate((rec_grad, rec_new, gate_grad, gate_new)):
        tile = jnp.where(row == i, square_sum(value), tile)
    for i in range(sums.shape[0]):
        sums[i] = tile


def update_kernel(
    sums,
    full,
    rec_weight,
    gate_weight,
    rec_new,
    rec_moment,
    rec_step,
    rec_copy,
    gate_new,
    gate_moment,
    gate_step,
    gate_copy,
):
    rep, rows, block = full.shape
    run = rec_weight.shape[0] // rep
    depth = rows - run
    half, share = block // 2, block // rep
    rec_value = full[:, pl.ds(0, run), :].reshape(rep * run, block)
    parts = []
    for q in range(2):
        part = None
        for r in range(rep):
            term = jnp.dot(
                full[r, pl.ds(run, depth), pl.ds(0, half)],
                placing(block, share, q, r),
                precision=HIGH,
                preferred_element_type=F32,
            )
            part = term if part is None else part + term
        parts.append(part)
    gate_value = jnp.concatenate(parts, axis=0)

    total = sums[0]
    for i in range(1, sums.shape[0]):
        total += sums[i]
    places = (
        (rec_value, rec_weight, rec_new, rec_moment, rec_step, rec_copy),
        (gate_value, gate_weight, gate_new, gate_moment, gate_step, gate_copy),
    )
    for i, (value, weight, new, moment, step, copy) in enumerate(places):
        scale = jnp.sqrt(total[2 * i : 2 * i + 1]) / jnp.sqrt(
            total[2 * i + 1 : 2 * i + 2] + EPSILON
        )
        scale = jnp.concatenate([LEARN_RATE * scale] * 2, axis=1)
        taken = scale * value
        result = weight[...] - taken
        moment[...] = value
        step[...] = taken
        new[...] = result
        copy[...] = result.astype(jnp.bfloat16)


def shards(
    normed,
    rec_cot,
    conv_out,
    gate_cot,
    rec_weight,
    rec_moment,
    rec_right,
    gate_weight,
    gate_moment,
    gate_left,
    gate_right,
):
    fs, rep = lax.axis_size("fs"), lax.axis_size("rep")
    like = lambda value, kind=F32: jax.ShapeDtypeStruct(value.shape, kind)
    gate_weight, gate_moment = gate_weight[0], gate_moment[0]

    with jax.named_scope("product"):
        tiles = product(normed, rec_cot, conv_out, gate_cot, gate_right[0], rep)
    with jax.named_scope("near"):
        arrived = exchange(tiles, "rep")
    with jax.named_scope("left"):
        left = lax.all_gather(gate_left[0].astype(F32), "fs", tiled=True).reshape(fs, *gate_left.shape[1:])
    with jax.named_scope("middle"):
        tiles = middle(arrived, left)
    with jax.named_scope("quarter"):
        hi, lo, cores = fs // SPAN, SPAN, lax.axis_size("tp_1")
        rows = tiles.shape[1]
        tiles = tiles.reshape(lo, hi * rows, -1)
        tiles = add_up(exchange(tiles, CORE, z_groups(fs, cores, True)))
    with jax.named_scope("far"):
        tiles = tiles.reshape(hi, rows, -1)
        arrived = exchange(tiles, CORE, z_groups(fs, cores, False))
    with jax.named_scope("settle"):
        mine, sums = on_core(
            settle_kernel,
            (
                jax.ShapeDtypeStruct(arrived.shape[1:], F32),
                jax.ShapeDtypeStruct((size_of(CORE), 4, 128), F32),
            ),
            (arrived, rec_right, rec_moment, gate_moment),
        )
    with jax.named_scope("share"):
        full = lax.all_gather(mine, "rep")
    with jax.named_scope("sums"):
        sums = fold(exchange(sums, CORE), size_of(PLANE), full)
        sums = exchange(sums, PLANE)
    with jax.named_scope("update"):
        bf16 = jnp.bfloat16
        (
            rec_new,
            rec_moment_new,
            rec_step,
            rec_copy,
            gate_new,
            gate_moment_new,
            gate_step,
            gate_copy,
        ) = on_core(
            update_kernel,
            (
                like(rec_weight),
                like(rec_weight),
                like(rec_weight),
                like(rec_weight, bf16),
                like(gate_weight),
                like(gate_weight),
                like(gate_weight),
                like(gate_weight, bf16),
            ),
            (sums, full, rec_weight, gate_weight),
        )
    return (
        rec_new,
        rec_moment_new,
        rec_step,
        rec_copy,
        gate_new[None],
        gate_moment_new[None],
        gate_step[None],
        gate_copy[None],
    )


def solution(mesh):
    fs, rep, tp = (mesh.shape[name] for name in ("fs", "rep", "tp"))
    split = Mesh(
        mesh.devices.reshape(fs, rep, tp // 2, 2),
        ("fs", "rep", *TP),
    )
    tokens = ("fs", "rep")
    placed = (
        P(tokens, None),
        P(tokens, TP),
        P(tokens, TP),
        P(tokens, TP),
        P("fs", TP),
        P("fs", TP),
        P(TP, None),
        P(TP, "fs", None),
        P(TP, "fs", None),
        P(TP, "fs", None),
        P(TP, None, None),
    )

    return jax.shard_map(
        shards,
        mesh=split,
        in_specs=placed,
        out_specs=(P("fs", TP),) * 4 + (P(TP, "fs", None),) * 4,
        check_vma=False,
    )
```
